128 devices in a mesh: sp: 64 (over z, y, x), tp: 2 (over core).
Axes of the slice: x: 4, y: 4, z: 4, core: 2. Of those that a mesh axis runs over, the one named last changes fastest.
Arguments:
- stream: bfloat16 [16384, 2048], P('sp', 'tp'), may hold values from -80 to 80
- norm_gain: float32 [2048], P('tp'), may hold values from 0.1 to 1.9
- cotangent: bfloat16 [16384, 2048], P('sp', 'tp'), may hold values from -16 to 16
- route_weights: float32 [16384, 2], P('sp'), may hold values from 0.1 to 1.5
- routes: int32 [16384, 2], P('sp'), may hold values from 0 to 63, all different within a row; in each aligned block of 256 rows (0 to 255, 256 to 511, ...) at most 16 rows name the same one
- conv_input: bfloat16 [16384, 1024], P('sp', 'tp'), may hold values from -6 to 6
- conv_bgate: bfloat16 [16384, 1024], P('sp', 'tp'), may hold values from -6 to 6
- conv_cgate: bfloat16 [16384, 1024], P('sp', 'tp'), may hold values from -6 to 6
- conv_taps: float32 [3, 1024], P(None, 'tp'), may hold values from -3 to 3
- out_proj: bfloat16 [2048, 1024], P(None, 'tp'), may hold values from -0.1875 to 0.1875
- gate_weight: bfloat16 [64, 2048, 1024], P('sp', None, 'tp'), may hold values from -0.125 to 0.125
- up_weight: bfloat16 [64, 2048, 1024], P('sp', None, 'tp'), may hold values from -0.125 to 0.125
- down_weight: bfloat16 [64, 1024, 2048], P('sp', 'tp'), may hold values from -0.1875 to 0.1875
Outputs:
- stream_grad: bfloat16 [16384, 2048], P('sp', 'tp')
- proj_grad: float32 [2048, 1024], P('sp', 'tp')
- input_grad: bfloat16 [16384, 1024], P('sp', 'tp')
- bgate_grad: bfloat16 [16384, 1024], P('sp', 'tp')
- cgate_grad: bfloat16 [16384, 1024], P('sp', 'tp')
- gate_grad: float32 [64, 2048, 1024], P('sp', None, 'tp')
- up_grad: float32 [64, 2048, 1024], P('sp', None, 'tp')
- down_grad: float32 [64, 1024, 2048], P('sp', 'tp')
The draws below stay inside these ranges and needn't reach their ends.
Inputs may be any that keep to these rules, and one draw needn't show every extreme that they name: `routes`: the 2 experts of a token differ. Among the tokens of one index of sp, no expert is named more than 16 times, a bound that some block reaches.
All inputs are finite; a program needn't handle non-finite values.
Results may differ from the reference program's by a relative error of at most 0.003.
The reference program's roundings to bfloat16 on the way count: a program that leaves them out, or rounds other values in their place, can miss the bound.
Values may be sent and summed in bfloat16 or wider, within the bound.
A program may use at most 128 MiB of HBM per device.

```python
import math
import jax
import jax.numpy as jnp
import numpy as np
from jax import lax

D = 2048
CW = 1024
EH = 1024
K = 2
TOK_DEV = 256
TOKENS = 16384
EXPERTS = 64
CAP = 16
N_SP = 64
N_TP = 2


def draw_stream(key, part):
    keys = jax.random.split(key, 3)
    row_scale = jnp.exp(jax.random.uniform(keys[0], (TOKENS, 1), jnp.float32, 0.0, 2.3))
    column_rise = 3.0 ** (jnp.arange(D, dtype=jnp.float32) / D)
    column_scale = column_rise[None, :] * jnp.exp(jax.random.uniform(keys[1], (1, D), jnp.float32, -0.5, 0.5))
    values = jax.random.normal(keys[2], (TOKENS, D), jnp.float32)
    return jnp.clip(values * row_scale * column_scale, -80.0, 80.0).astype(jnp.bfloat16)


def spiked(array, key, source, target, parts, factor):
    def block_of(axis_at):
        return (jnp.arange(array.shape[axis_at]) // (array.shape[axis_at] // parts)).reshape((-1,) + (1,) * (array.ndim - 1 - axis_at))

    one_side = jax.random.permutation(key, parts)[block_of(target)]
    other_side = (block_of(target) + parts // 2) % parts
    return jnp.where((block_of(source) == one_side) | (block_of(source) == other_side), factor * array, array)


def steps_of(key, extent, shards, smallest, top_value):
    gain, own = 1.0, jax.random.fold_in(key, 6)
    for dim, parts in shards:
        steps = jnp.exp(jax.random.uniform(jax.random.fold_in(own, dim), (parts,), jnp.float32, smallest / len(shards), top_value / len(shards)))
        gain = gain * jnp.repeat(steps, extent[dim] // parts).reshape([-1 if axis == dim else 1 for axis in range(len(extent))])
    return gain


def shared_out(rng, own, number, rows, count, top, limit, slope):
    ranking = jax.random.permutation(rng, count)
    packed, ordinary = portions_of(count, rows * top, limit, slope, True), portions_of(count, rows * top, limit, slope, False)
    places = jnp.arange(count)

    def named(lengths, turn):
        used = int((lengths > 0).sum())
        fixed = max(1, used // 4)
        shifted = fixed + (places - fixed + turn * (used - fixed)) % max(1, count - fixed)
        return jnp.zeros((count,), jnp.int32).at[ranking[jnp.where(places < fixed, places, shifted)]].set(jnp.asarray(lengths, jnp.int32))

    lengths = jnp.where(number % 4 == 0, named(packed, number // 4), named(ordinary, number - number // 4 - 1))
    mixed = jax.random.permutation(jax.random.fold_in(own, 3), count)
    source_of, sink = mixed[0:count // 2 * 2:2], mixed[1:count // 2 * 2:2]
    room = jnp.minimum(lengths[source_of] - 1, limit - lengths[sink]) // 2
    room = jnp.where((source_of == ranking[0]) | (sink == ranking[0]) | (lengths[sink] == 0), 0, jnp.maximum(room, 0))
    shifted = jax.random.randint(jax.random.fold_in(own, 4), (count // 2,), 0, 1 << 20) % (room + 1)
    lengths = lengths.at[source_of].add(-shifted).at[sink].add(shifted)
    members = jnp.searchsorted(jnp.cumsum(lengths), jnp.arange(rows * top), side="right").astype(jnp.int32)
    grid = members.reshape(top, rows).T
    grid = grid[jax.random.permutation(jax.random.fold_in(own, 1), rows)]
    turn = jax.random.randint(jax.random.fold_in(own, 2), (rows, 1), 0, top)
    return jnp.take_along_axis(grid, (jnp.arange(top)[None, :] + turn) % top, axis=1)


def portions_of(amount, total, bound, lean, full):
    loads = [(1 << 20) // math.isqrt(standing ** lean) + 1 for standing in range(1, amount + 1)]
    largest = bound if full else min(bound, max(-(-total // amount), total * loads[0] // sum(loads)))
    least = 1 if total - largest >= amount - 1 else 0
    given, spare = [largest] + [least] * (amount - 1), total - largest - least * (amount - 1)
    while spare > 0:
        candidates = [i for i in range(1, amount) if given[i] < largest] or [i for i in range(1, amount) if given[i] < bound]
        mass, left = sum([loads[i] for i in candidates]), spare
        for i in candidates:
            extra = min(bound - given[i], max(1, left * loads[i] // mass), spare)
            given[i] = given[i] + extra
            spare = spare - extra
    return np.array(given)


def gaussian(stream_key, extent, spread, limit, pieces=(), kind=jnp.bfloat16):
    loudness = steps_of(stream_key, extent, pieces, -0.22, 0.18) if pieces else 1.0
    result = jax.random.normal(stream_key, extent, jnp.float32) * spread * loudness
    return jnp.minimum(jnp.maximum(result, -limit), limit).astype(kind)


def noise_with(own_key, extent, scale, bound, pieces, heavy, kind=jnp.bfloat16):
    entries = scale * jax.random.normal(own_key, extent, jnp.float32)
    if pieces:
        entries = entries * steps_of(own_key, extent, pieces, -0.22, 0.18)
    return jnp.clip(spiked(entries, jax.random.fold_in(own_key, 3), *heavy), -bound, bound).astype(kind)


def setup_inputs(seed: int = 0) -> dict:
    splits = jax.random.split(jax.random.key(seed), 14)
    stream = draw_stream(jax.random.fold_in(splits[13], 71), 0)
    norm_gain = jnp.clip(1.0 + 0.18 * jax.random.normal(splits[1], (D,), jnp.float32), 0.1, 1.9)
    cotangent = noise_with(splits[2], (TOKENS, D), 1.0, 16.0, ((0, 64), (1, 2)), (0, 1, 64, 4.0))
    route_weights = jnp.clip(0.1 + 1.4 * jax.random.uniform(splits[3], (TOKENS, K), jnp.float32) ** steps_of(splits[3], (TOKENS, K), ((0, 64),), -0.2, 0.2), 0.1, 1.5)
    routes_keys = jax.random.split(jax.random.fold_in(splits[4], 1), TOKENS // TOK_DEV)
    routes_turns = jax.random.permutation(jax.random.fold_in(splits[4], 3), TOKENS // TOK_DEV)
    routes = jax.vmap(lambda own, number: shared_out(jax.random.fold_in(splits[4], 2), own, number, TOK_DEV, EXPERTS, K, CAP, 1))(routes_keys, routes_turns).reshape((TOKENS, K))
    conv_input = gaussian(splits[5], (TOKENS, CW), 1.0, 6.0, ((0, 64), (1, 2)))
    conv_bgate = gaussian(splits[6], (TOKENS, CW), 1.0, 6.0, ((0, 64), (1, 2)))
    conv_cgate = gaussian(splits[7], (TOKENS, CW), 1.0, 6.0, ((0, 64), (1, 2)))
    conv_taps = gaussian(splits[8], (3, CW), 0.5, 3.0, ((1, 2),), jnp.float32)
    out_proj = gaussian(splits[9], (D, CW), CW ** -0.5, 0.1875, ((1, 2),))
    gate_weight = gaussian(splits[10], (EXPERTS, D, EH), D ** -0.5, 0.125, ((0, 64), (2, 2)))
    up_weight = gaussian(splits[11], (EXPERTS, D, EH), D ** -0.5, 0.125, ((0, 64), (2, 2)))
    down_weight = gaussian(splits[12], (EXPERTS, EH, D), EH ** -0.5, 0.1875, ((0, 64), (1, 2)))
    return {"stream": stream, "norm_gain": norm_gain, "cotangent": cotangent, "route_weights": route_weights, "routes": routes, "conv_input": conv_input, "conv_bgate": conv_bgate, "conv_cgate": conv_cgate, "conv_taps": conv_taps, "out_proj": out_proj, "gate_weight": gate_weight, "up_weight": up_weight, "down_weight": down_weight}


EPSILON = 1e-06

def expert_backward(inputs, grads_out, gate_w, up_w, down_w):
    gate_lin = jnp.dot(inputs, gate_w, preferred_element_type=jnp.float32)
    up_lin = jnp.dot(inputs, up_w, preferred_element_type=jnp.float32)
    sigmoid_gate = jax.nn.sigmoid(gate_lin)
    silu_gate = gate_lin * sigmoid_gate
    hidden = (silu_gate * up_lin).astype(jnp.bfloat16)
    down_g = jnp.dot(hidden.T, grads_out, preferred_element_type=jnp.float32)
    hidden_grad = jnp.dot(grads_out, down_w.T, preferred_element_type=jnp.float32)
    gate_pre = (hidden_grad * up_lin * sigmoid_gate * (1.0 + gate_lin * (1.0 - sigmoid_gate))).astype(jnp.bfloat16)
    up_pre = (hidden_grad * silu_gate).astype(jnp.bfloat16)
    gate_g = jnp.dot(inputs.T, gate_pre, preferred_element_type=jnp.float32)
    up_g = jnp.dot(inputs.T, up_pre, preferred_element_type=jnp.float32)
    return (gate_g, up_g, down_g, gate_pre, up_pre)

def reference(stream, norm_gain, cotangent, route_weights, routes, conv_input, conv_bgate, conv_cgate, conv_taps, out_proj, gate_weight, up_weight, down_weight):
    stream_float = stream.astype(jnp.float32)
    inverse = lax.rsqrt(lax.optimization_barrier(jnp.mean(stream_float * stream_float, axis=1, keepdims=True)) + EPSILON)
    normed = (stream_float * inverse * norm_gain[None, :]).astype(jnp.bfloat16)
    cot_float = cotangent.astype(jnp.float32)
    weighted = (route_weights[:, :, None] * cot_float[:, None, :]).astype(jnp.bfloat16).reshape(TOKENS * K, D)
    blocks = routes.reshape(N_SP, TOK_DEV * K).astype(jnp.int32)
    onehot = (blocks[:, :, None] == jnp.arange(EXPERTS, dtype=jnp.int32)[None, None, :]).astype(jnp.int32)
    earlier = jnp.cumsum(onehot, axis=1) - onehot
    position = lax.optimization_barrier(jnp.sum(earlier * onehot, axis=2)).astype(jnp.int32)
    source = jnp.arange(N_SP, dtype=jnp.int32)[:, None]
    arrival = (source * CAP + position).astype(jnp.int32)
    assign_ids = jnp.arange(TOKENS * K, dtype=jnp.int32).reshape(N_SP, TOK_DEV * K)
    table = jnp.full((EXPERTS, N_SP * CAP), TOKENS * K, jnp.int32).at[blocks, arrival].set(assign_ids)
    normed_pad = jnp.concatenate([normed, jnp.zeros((1, D), jnp.bfloat16)], axis=0)
    weighted_pad = jnp.concatenate([weighted, jnp.zeros((1, D), jnp.bfloat16)], axis=0)
    half_width = EH // N_TP

    def one_expert(operands):
        slot_ids, gate_w, up_w, down_w = operands
        token_ids = (slot_ids // K).astype(jnp.int32)
        inputs = normed_pad[token_ids]
        grads_out = weighted_pad[slot_ids]
        gate_g, up_g, down_g, gate_pre, up_pre = expert_backward(inputs, grads_out, gate_w, up_w, down_w)
        summed = jnp.zeros((N_SP * CAP, D), jnp.float32)
        for part_index in range(N_TP):
            low_col = part_index * half_width
            partial_value = jnp.dot(gate_pre[:, low_col:low_col + half_width], gate_w[:, low_col:low_col + half_width].T, preferred_element_type=jnp.float32)
            partial_value = partial_value + jnp.dot(up_pre[:, low_col:low_col + half_width], up_w[:, low_col:low_col + half_width].T, preferred_element_type=jnp.float32)
            rounded = lax.optimization_barrier(partial_value.astype(jnp.bfloat16))
            summed = summed + rounded.astype(jnp.float32)
        return (gate_g, up_g, down_g, summed.astype(jnp.bfloat16))
    gate_grad, up_grad, down_grad, slot_grads = lax.map(one_expert, (table, gate_weight, up_weight, down_weight))
    token_index = (table.reshape(-1) // K).astype(jnp.int32)
    normed_grad = jnp.zeros((TOKENS + 1, D), jnp.float32).at[token_index].add(slot_grads.reshape(-1, D).astype(jnp.float32))[:TOKENS]
    cross = lax.optimization_barrier(jnp.sum(stream_float * norm_gain[None, :] * normed_grad, axis=1, keepdims=True))
    stream_grad = (cot_float + inverse * norm_gain[None, :] * normed_grad - stream_float * inverse * inverse * inverse * cross / D).astype(jnp.bfloat16)
    input_float = conv_input.astype(jnp.float32)
    cgate_float = conv_cgate.astype(jnp.float32)
    bgate_float = conv_bgate.astype(jnp.float32)
    gated = cgate_float * input_float
    padded = jnp.pad(gated, ((2, 0), (0, 0)))
    conv_out = conv_taps[0][None, :] * padded[:-2] + conv_taps[1][None, :] * padded[1:-1] + conv_taps[2][None, :] * padded[2:]
    mixer_out = (bgate_float * conv_out).astype(jnp.bfloat16)
    proj_grad = lax.dot_general(stream_grad, mixer_out, (((0,), (0,)), ((), ())), preferred_element_type=jnp.float32)
    mixer_grad = jnp.dot(stream_grad, out_proj, preferred_element_type=jnp.float32)
    delta = mixer_grad * bgate_float
    padded_back = jnp.pad(delta, ((0, 2), (0, 0)))
    gated_grad = conv_taps[2][None, :] * padded_back[:-2] + conv_taps[1][None, :] * padded_back[1:-1] + conv_taps[0][None, :] * padded_back[2:]
    bgate_grad = (mixer_grad * conv_out).astype(jnp.bfloat16)
    input_grad = (gated_grad * cgate_float).astype(jnp.bfloat16)
    cgate_grad = (gated_grad * input_float).astype(jnp.bfloat16)
    return (stream_grad, proj_grad, input_grad, bgate_grad, cgate_grad, gate_grad, up_grad, down_grad)
```

```python
import functools

import jax
import jax.numpy as jnp
from jax import lax
from jax.experimental import pallas as pl
from jax.experimental.pallas import tpu as pltpu
from jax.sharding import PartitionSpec as P

D = 2048
EPSILON = 1e-06
MESH = pl.DeviceIdType.MESH
SIDE = 4
CHIPS = SIDE**3


def _parts(k):
    return k // 16, (k // 4) % 4, k % 4


def _join(z, y, x):
    return (z % 4) * 16 + (y % 4) * 4 + x % 4


def _shift_order():
    hops = lambda k: sum(min(a, SIDE - a) for a in _parts(k))
    turn = lambda k: _join(*(_parts(k)[1:] + _parts(k)[:1]))
    back = lambda k: _join(*(-a for a in _parts(k)))
    order = []
    for k in sorted(range(1, CHIPS), key=lambda k: -hops(k)):
        for kk in (k, turn(k), turn(turn(k))):
            for other in (kk,):
                if other not in order:
                    order.append(other)
        for kk in (k, turn(k), turn(turn(k))):
            if back(kk) not in order:
                order.append(back(kk))
    return order


ORDER = _shift_order()


def moved(me, k, sign=1):
    z, y, x = me // 16, lax.rem(me // 4, 4), lax.rem(me, 4)
    kz, ky, kx = (a if sign > 0 else (SIDE - a) % SIDE for a in _parts(k))
    return lax.rem(z + kz, 4) * 16 + lax.rem(y + ky, 4) * 4 + lax.rem(x + kx, 4)


def greet_all(me, core, partner):
    barrier = pltpu.get_barrier_semaphore()
    for k in ORDER:
        pl.semaphore_signal(
            barrier, inc=1, device_id=(moved(me, k), core), device_id_type=MESH
        )
    count = CHIPS - 1
    if partner:
        pl.semaphore_signal(barrier, inc=1, device_id=(me, 1 - core), device_id_type=MESH)
        count += 1
    pl.semaphore_wait(barrier, count)


def dispatch_kernel(group, send, out, send_sem, recv_sem, pass_send, pass_recv):
    me, core = lax.axis_index("sp"), lax.axis_index("tp")
    greet_all(me, core, True)
    copies = []
    for j, k in enumerate(ORDER):
        peer = moved(me, k)
        copy = pltpu.make_async_remote_copy(
            src_ref=send.at[peer],
            dst_ref=out.at[core, j],
            send_sem=send_sem.at[j],
            recv_sem=recv_sem.at[j],
            device_id=(peer, core),
            device_id_type=MESH,
        )
        copy.start()
        copies.append(copy)
    out[core, CHIPS - 1] = send[me]
    passes = []
    for g in range(CHIPS // group):
        for j in range(g * group, (g + 1) * group):
            if j < CHIPS - 1:
                copies[j].wait_recv()
        onward = pltpu.make_async_remote_copy(
            src_ref=out.at[core, pl.ds(g * group, group)],
            dst_ref=out.at[core, pl.ds(g * group, group)],
            send_sem=pass_send.at[g],
            recv_sem=pass_recv.at[g],
            device_id=(me, 1 - core),
            device_id_type=MESH,
        )
        onward.start()
        passes.append(onward)
    for onward in passes:
        onward.wait()
    for copy in copies:
        copy.wait_send()


def dispatch(send):
    rows, columns = send.shape[1:]
    group = 8
    vmem = pl.BlockSpec(memory_space=pltpu.VMEM)
    return pl.pallas_call(
        functools.partial(dispatch_kernel, group),
        out_shape=jax.ShapeDtypeStruct((2, CHIPS, rows, columns), send.dtype),
        in_specs=[vmem],
        out_specs=vmem,
        scratch_shapes=[
            pltpu.SemaphoreType.DMA((CHIPS,)),
            pltpu.SemaphoreType.DMA((CHIPS,)),
            pltpu.SemaphoreType.DMA((CHIPS // group,)),
            pltpu.SemaphoreType.DMA((CHIPS // group,)),
        ],
        compiler_params=pltpu.CompilerParams(
            collective_id=0, has_side_effects=True, vmem_limit_bytes=40 << 20
        ),
        name="dispatch",
    )(send)


def swap_kernel(backward, send, out, send_sem, recv_sem):
    me, core = lax.axis_index("sp"), lax.axis_index("tp")
    greet_all(me, core, False)
    copies = []
    for j, k in enumerate(ORDER):
        peer = moved(me, k, -1 if backward else 1)
        copy = pltpu.make_async_remote_copy(
            src_ref=send.at[j if backward else peer],
            dst_ref=out.at[me if backward else j],
            send_sem=send_sem.at[j],
            recv_sem=recv_sem.at[j],
            device_id=(peer, core),
            device_id_type=MESH,
        )
        copy.start()
        copies.append(copy)
    if backward:
        out[me] = send[CHIPS - 1]
    else:
        out[CHIPS - 1] = send[me]
    for copy in copies:
        copy.wait()


def swap(send, backward, collective_id, name):
    vmem = pl.BlockSpec(memory_space=pltpu.VMEM)
    return pl.pallas_call(
        functools.partial(swap_kernel, backward),
        out_shape=jax.ShapeDtypeStruct(send.shape, send.dtype),
        in_specs=[vmem],
        out_specs=vmem,
        scratch_shapes=[
            pltpu.SemaphoreType.DMA((CHIPS,)),
            pltpu.SemaphoreType.DMA((CHIPS,)),
        ],
        compiler_params=pltpu.CompilerParams(
            collective_id=collective_id, has_side_effects=True, vmem_limit_bytes=24 << 20
        ),
        name=name,
    )(send)


def gathered_total(array, axis):
    return lax.all_gather(array, axis).sum(0)


def sent_and_summed(array, axis, dim):
    dims = array.shape
    length = lax.axis_size(axis)
    parts = array.reshape(*dims[:dim], length, dims[dim] // length, *dims[dim + 1 :])
    parts = jnp.moveaxis(parts, dim, 0)
    arrived = lax.all_to_all(parts, axis, split_axis=0, concat_axis=0, tiled=True)
    return arrived.astype(jnp.float32).sum(axis=0)


def gathered_copies(array, axis, dim):
    copies = jnp.broadcast_to(array, (lax.axis_size(axis), *array.shape))
    parts = lax.all_to_all(copies, axis, split_axis=0, concat_axis=0, tiled=True)
    return jnp.concatenate([parts[0], parts[1]], axis=dim)


def shifted(value, axis, steps):
    count = lax.axis_size(axis)
    leading, last = (max(0, -steps), min(count, count - steps))
    return lax.ppermute(value, axis, [(source, source + steps) for source in range(leading, last)])


def slot_matrix(routes, experts, capacity):
    assigned = routes.reshape(-1)
    onehot = (assigned[:, None] == jnp.arange(experts, dtype=jnp.int32)[None, :]).astype(jnp.int32)
    earlier = jnp.cumsum(onehot, axis=0) - onehot
    position = jnp.sum(earlier * onehot, axis=1)
    target = assigned * capacity + position
    places = jnp.arange(experts * capacity, dtype=jnp.int32)
    return (places[:, None] == target[None, :]).astype(jnp.bfloat16)


def select_rows(selector, values):
    return jnp.dot(selector, values, preferred_element_type=jnp.float32).astype(jnp.bfloat16)


def contract_rows(left, right):
    return lax.dot_general(
        left, right, (((0,), (0,)), ((), ())), preferred_element_type=jnp.float32
    )


def contract_cols(left, right):
    return lax.dot_general(
        left, right, (((1,), (1,)), ((), ())), preferred_element_type=jnp.float32
    )


def local(
    stream,
    norm_gain,
    cotangent,
    route_weights,
    routes,
    conv_input,
    conv_bgate,
    conv_cgate,
    conv_taps,
    out_proj,
    gate_weight,
    up_weight,
    down_weight,
):
    experts = lax.axis_size("sp")
    tok_count = stream.shape[0]
    top_count = routes.shape[1]
    capacity = 2 * tok_count * top_count // experts
    half = stream.shape[1]
    stream_float = stream.astype(jnp.float32)
    square_sum = gathered_total(jnp.sum(stream_float * stream_float, axis=1), "tp")
    inverse = lax.rsqrt(square_sum / D + EPSILON)[:, None]
    gain_row = norm_gain[None, :]
    normed = (stream_float * inverse * gain_row).astype(jnp.bfloat16)
    cot_float = cotangent.astype(jnp.float32)
    weighted = (route_weights[:, :, None] * cot_float[:, None, :]).astype(jnp.bfloat16)
    weighted = weighted.reshape(tok_count * top_count, -1)
    selector = slot_matrix(routes, experts, capacity)
    token_select = jnp.sum(selector.reshape(experts * capacity, tok_count, top_count), axis=2)
    send_inputs = select_rows(token_select, normed)
    send_grads = select_rows(selector, weighted)
    send = jnp.concatenate([send_inputs, send_grads], axis=1)
    arrived = dispatch(send.reshape(experts, capacity, 2 * half))
    arrived = arrived.reshape(2, experts * capacity, 2 * half)
    recv_inputs = jnp.concatenate([arrived[0, :, :half], arrived[1, :, :half]], axis=1)
    recv_grads = jnp.concatenate([arrived[0, :, half:], arrived[1, :, half:]], axis=1)
    gate_w = gate_weight[0]
    up_w = up_weight[0]
    down_w = down_weight[0]
    gate_lin = jnp.dot(recv_inputs, gate_w, preferred_element_type=jnp.float32)
    up_lin = jnp.dot(recv_inputs, up_w, preferred_element_type=jnp.float32)
    sigmoid_gate = jax.nn.sigmoid(gate_lin)
    silu_gate = gate_lin * sigmoid_gate
    hidden = (silu_gate * up_lin).astype(jnp.bfloat16)
    down_g = contract_rows(hidden, recv_grads)
    hidden_grad = contract_cols(recv_grads, down_w)
    gate_pre = (
        hidden_grad * up_lin * sigmoid_gate * (1.0 + gate_lin * (1.0 - sigmoid_gate))
    ).astype(jnp.bfloat16)
    up_pre = (hidden_grad * silu_gate).astype(jnp.bfloat16)
    gate_g = contract_rows(recv_inputs, gate_pre)
    up_g = contract_rows(recv_inputs, up_pre)
    partial_value = contract_cols(gate_pre, gate_w) + contract_cols(up_pre, up_w)
    rounded = lax.optimization_barrier(partial_value.astype(jnp.bfloat16))
    summed = sent_and_summed(rounded.astype(jnp.float32).astype(jnp.bfloat16), "tp", 1)
    row_grads = summed.astype(jnp.bfloat16)
    returned = swap(row_grads.reshape(experts, capacity, half), True, 1, "give_back")
    returned = returned.reshape(experts * capacity, half)
    normed_grad = contract_rows(token_select, returned)
    cross = gathered_total(jnp.sum(stream_float * gain_row * normed_grad, axis=1), "tp")
    stream_grad = (
        cot_float
        + inverse * gain_row * normed_grad
        - stream_float * inverse * inverse * inverse * cross[:, None] / D
    ).astype(jnp.bfloat16)
    grad_whole = gathered_copies(stream_grad, "tp", 1)
    input_float = conv_input.astype(jnp.float32)
    cgate_float = conv_cgate.astype(jnp.float32)
    bgate_float = conv_bgate.astype(jnp.float32)
    rim_rows = shifted(jnp.stack([conv_input[-2:], conv_cgate[-2:]]), "sp", 1)
    rim_gated = rim_rows[1].astype(jnp.float32) * rim_rows[0].astype(jnp.float32)
    gated = cgate_float * input_float
    extended = jnp.concatenate([rim_gated, gated], axis=0)
    conv_out = (
        conv_taps[0][None, :] * extended[:-2]
        + conv_taps[1][None, :] * extended[1:-1]
        + conv_taps[2][None, :] * extended[2:]
    )
    mixer_out = (bgate_float * conv_out).astype(jnp.bfloat16)
    shares = contract_rows(grad_whole, mixer_out).astype(jnp.bfloat16)
    shares = swap(shares.reshape(experts, D // experts, -1), False, 2, "share")
    proj_grad = shares.astype(jnp.float32).sum(axis=0)
    mixer_grad = jnp.dot(grad_whole, out_proj, preferred_element_type=jnp.float32)
    delta = mixer_grad * bgate_float
    next_rim = shifted(delta[:2], "sp", -1)
    extended_back = jnp.concatenate([delta, next_rim], axis=0)
    gated_grad = (
        conv_taps[2][None, :] * extended_back[:-2]
        + conv_taps[1][None, :] * extended_back[1:-1]
        + conv_taps[0][None, :] * extended_back[2:]
    )
    bgate_grad = (mixer_grad * conv_out).astype(jnp.bfloat16)
    input_grad = (gated_grad * cgate_float).astype(jnp.bfloat16)
    cgate_grad = (gated_grad * input_float).astype(jnp.bfloat16)
    return (
        stream_grad,
        proj_grad,
        input_grad,
        bgate_grad,
        cgate_grad,
        gate_g[None],
        up_g[None],
        down_g[None],
    )


def solution(mesh):
    return jax.shard_map(
        local,
        mesh=mesh,
        in_specs=(
            P("sp", "tp"),
            P("tp"),
            P("sp", "tp"),
            P("sp", None),
            P("sp", None),
            P("sp", "tp"),
            P("sp", "tp"),
            P("sp", "tp"),
            P(None, "tp"),
            P(None, "tp"),
            P("sp", None, "tp"),
            P("sp", None, "tp"),
            P("sp", "tp", None),
        ),
        out_specs=(
            P("sp", "tp"),
            P("sp", "tp"),
            P("sp", "tp"),
            P("sp", "tp"),
            P("sp", "tp"),
            P("sp", None, "tp"),
            P("sp", None, "tp"),
            P("sp", "tp", None),
        ),
        check_vma=False,
    )
```

```python
import functools

import jax
import jax.numpy as jnp
from jax import lax
from jax.experimental import pallas as pl
from jax.experimental.pallas import tpu as pltpu
from jax.sharding import PartitionSpec as P

D = 2048
EPSILON = 1e-06
MESH = pl.DeviceIdType.MESH
SIDE = 4
CHIPS = SIDE**3


def _parts(k):
    return k // 16, (k // 4) % 4, k % 4


def _join(z, y, x):
    return (z % 4) * 16 + (y % 4) * 4 + x % 4


def _shift_order():
    hops = lambda k: sum(min(a, SIDE - a) for a in _parts(k))
    turn = lambda k: _join(*(_parts(k)[1:] + _parts(k)[:1]))
    back = lambda k: _join(*(-a for a in _parts(k)))
    order = []
    for k in sorted(range(1, CHIPS), key=lambda k: -hops(k)):
        for kk in (k, turn(k), turn(turn(k))):
            for other in (kk,):
                if other not in order:
                    order.append(other)
        for kk in (k, turn(k), turn(turn(k))):
            if back(kk) not in order:
                order.append(back(kk))
    return order


ORDER = _shift_order()


def moved(me, k, sign=1):
    z, y, x = me // 16, lax.rem(me // 4, 4), lax.rem(me, 4)
    kz, ky, kx = (a if sign > 0 else (SIDE - a) % SIDE for a in _parts(k))
    return lax.rem(z + kz, 4) * 16 + lax.rem(y + ky, 4) * 4 + lax.rem(x + kx, 4)


GROUPS = 8
BLOCKS = CHIPS // GROUPS


def greet_all(me, core):
    barrier = pltpu.get_barrier_semaphore()
    for k in ORDER:
        pl.semaphore_signal(
            barrier, inc=1, device_id=(moved(me, k), core), device_id_type=MESH
        )
    pl.semaphore_signal(barrier, inc=1, device_id=(me, 1 - core), device_id_type=MESH)
    return barrier


def remote(source, target, send_sem, recv_sem, peer):
    return pltpu.make_async_remote_copy(
        src_ref=source,
        dst_ref=target,
        send_sem=send_sem,
        recv_sem=recv_sem,
        device_id=peer,
        device_id_type=MESH,
    )


def wait_for(ref, sem):
    pltpu.make_async_copy(ref, ref, sem).wait()


def dot(left, right, over=(1, 0)):
    return lax.dot_general(
        left, right, (((over[0],), (over[1],)), ((), ())), preferred_element_type=jnp.float32
    )


def experts_kernel(
    routes,
    weights,
    stream,
    gain,
    cot,
    gate_hbm,
    up_hbm,
    down_hbm,
    normed_grad,
    inverse_out,
    gate_g,
    up_g,
    down_g,
    gate_w,
    up_w,
    down_w,
    square,
    normed,
    select,
    send,
    rows_in,
    pre,
    hid,
    theirs,
    mine,
    other,
    ret,
    back,
    load_sem,
    square_sem,
    send_sem,
    recv_sem,
    pass_send,
    pass_recv,
    part_send,
    part_recv,
    back_send,
    back_recv,
):
    me, core = lax.axis_index("sp"), lax.axis_index("tp")
    partner = (me, 1 - core)
    capacity = send.shape[0] // CHIPS
    half = stream.shape[1]
    depth = BLOCKS * capacity
    width = gate_w.shape[1]
    barrier = greet_all(me, core)
    loads = [
        pltpu.make_async_copy(a, b, load_sem.at[i])
        for i, (a, b) in enumerate(((gate_hbm, gate_w), (up_hbm, up_w), (down_hbm, down_w)))
    ]
    for load in loads:
        load.start()
    stream_float = stream[...].astype(jnp.float32)
    part = jnp.sum(stream_float * stream_float, axis=1, keepdims=True)
    square[0] = jnp.broadcast_to(part, square.shape[1:])
    pl.semaphore_wait(barrier, CHIPS)
    swap = remote(square.at[0], square.at[1], square_sem.at[0], square_sem.at[1], partner)
    swap.start()

    tokens = stream.shape[0]
    first, second = routes[0:1, :], routes[1:2, :]
    expert = lax.broadcasted_iota(jnp.int32, (CHIPS, tokens), 0)
    on_first, on_second = expert == first, expert == second
    named = jnp.where(on_first | on_second, 1.0, 0.0).astype(jnp.bfloat16)
    before = lax.broadcasted_iota(jnp.int32, (tokens, tokens), 0) < lax.broadcasted_iota(
        jnp.int32, (tokens, tokens), 1
    )
    earlier = dot(named, jnp.where(before, 1.0, 0.0).astype(jnp.bfloat16))

    def target_of(on, route):
        rank = jnp.sum(jnp.where(on, earlier, 0.0), axis=0, keepdims=True)
        return route * capacity + rank.astype(jnp.int32)

    first_target, second_target = target_of(on_first, first), target_of(on_second, second)
    chunk = 256
    slot_weights = []
    for at in range(0, CHIPS * capacity, chunk):
        place = lax.broadcasted_iota(jnp.int32, (chunk, tokens), 0) + at
        is_first, is_second = place == first_target, place == second_target
        select[at : at + chunk] = jnp.where(is_first | is_second, 1.0, 0.0).astype(jnp.bfloat16)
        slot_weights.append(
            jnp.sum(
                jnp.where(is_first, weights[0:1, :], 0.0)
                + jnp.where(is_second, weights[1:2, :], 0.0),
                axis=1,
                keepdims=True,
            )
        )
    swap.wait()
    inverse = lax.rsqrt((square[0, :, 0:1] + square[1, :, 0:1]) / D + EPSILON)
    inverse_out[...] = jnp.broadcast_to(inverse, inverse_out.shape)
    normed[...] = (stream_float * inverse * gain[...]).astype(jnp.bfloat16)
    for i, at in enumerate(range(0, CHIPS * capacity, chunk)):
        chosen = select[at : at + chunk]
        send[at : at + chunk, :half] = dot(chosen, normed[...]).astype(jnp.bfloat16)
        send[at : at + chunk, half:] = (slot_weights[i] * dot(chosen, cot[...])).astype(
            jnp.bfloat16
        )

    def block(index):
        return pl.ds(pl.multiple_of(index * capacity, capacity), capacity)

    for j, k in enumerate(ORDER):
        peer = moved(me, k)
        remote(
            send.at[block(peer)],
            rows_in.at[core, pl.ds(j * capacity, capacity)],
            send_sem,
            recv_sem.at[j // BLOCKS],
            (peer, core),
        ).start()
    rows_in[core, (CHIPS - 1) * capacity :] = send[block(me)]
    for load in loads:
        load.wait()

    def group(g, count=depth):
        return pl.ds(pl.multiple_of(g * depth, depth), count)

    def passing(g):
        piece = rows_in.at[core, group(g)]
        return remote(piece, piece, pass_send.at[g], pass_recv.at[g], partner)

    def exchange(g):
        return remote(
            theirs.at[group(g)], other.at[group(g)], part_send.at[g], part_recv.at[g], partner
        )

    def take(g):
        @pl.when(g < GROUPS - 1)
        def _():
            wait_for(rows_in.at[core, group(g)], recv_sem.at[g])

        @pl.when(g == GROUPS - 1)
        def _():
            wait_for(rows_in.at[core, group(g, depth - capacity)], recv_sem.at[g])

        passing(g).start()

    def compute(g):
        wait_for(rows_in.at[1 - core, group(g)], pass_recv.at[g])
        rows = group(g)
        gate_lin = dot(rows_in[0, rows, :half], gate_w[:half]) + dot(
            rows_in[1, rows, :half], gate_w[half:]
        )
        up_lin = dot(rows_in[0, rows, :half], up_w[:half]) + dot(
            rows_in[1, rows, :half], up_w[half:]
        )
        hidden_grad = dot(rows_in[0, rows, half:], down_w[:, :half], (1, 1)) + dot(
            rows_in[1, rows, half:], down_w[:, half:], (1, 1)
        )
        sigmoid_gate = jax.nn.sigmoid(gate_lin)
        silu_gate = gate_lin * sigmoid_gate
        hid[rows] = (silu_gate * up_lin).astype(jnp.bfloat16)
        gate_pre = (
            hidden_grad * up_lin * sigmoid_gate * (1.0 + gate_lin * (1.0 - sigmoid_gate))
        ).astype(jnp.bfloat16)
        up_pre = (hidden_grad * silu_gate).astype(jnp.bfloat16)
        pre[rows, :width] = gate_pre
        pre[rows, width:] = up_pre
        for target, side in ((theirs, 1 - core), (mine, core)):
            features = pl.ds(pl.multiple_of(side * half, half), half)
            value = dot(gate_pre, gate_w[features], (1, 1)) + dot(up_pre, up_w[features], (1, 1))
            target[rows] = value.astype(jnp.bfloat16)
        exchange(g).start()

    def finish(g):
        wait_for(other.at[group(g)], part_recv.at[g])
        rows = group(g)
        ret[rows] = (mine[rows].astype(jnp.float32) + other[rows].astype(jnp.float32)).astype(
            jnp.bfloat16
        )
        for i in range(BLOCKS):
            k = jnp.int32(ORDER[i])
            for later in range(1, GROUPS):
                if later * BLOCKS + i < CHIPS - 1:
                    k = jnp.where(g == later, ORDER[later * BLOCKS + i], k)
            z = lax.rem(me // 16 + 4 - k // 16, 4)
            y = lax.rem(lax.rem(me // 4, 4) + 4 - lax.rem(k // 4, 4), 4)
            x = lax.rem(lax.rem(me, 4) + 4 - lax.rem(k, 4), 4)
            go = remote(
                ret.at[block(g * BLOCKS + i)],
                back.at[block(me)],
                back_send,
                back_recv,
                (z * 16 + y * 4 + x, core),
            )
            if i < BLOCKS - 1:
                go.start()
            else:
                pl.when(g < GROUPS - 1)(go.start)

    def step(i, carry):
        pl.when(i < GROUPS)(lambda: take(i))
        pl.when((i >= 1) & (i <= GROUPS))(lambda: compute(i - 1))
        pl.when(i >= 2)(lambda: finish(i - 2))
        return carry

    lax.fori_loop(0, GROUPS + 2, step, 0)
    back[block(me)] = ret[(CHIPS - 1) * capacity :]

    tile = 256

    def gate_step(i, carry):
        side, at = i // (half // tile), lax.rem(i, half // tile)
        columns = pl.ds(pl.multiple_of(at * tile, tile), tile)
        value = dot(rows_in[side, :, columns], pre[...], (0, 0))
        features = pl.ds(pl.multiple_of(i * tile, tile), tile)
        gate_g[features] = value[:, :width]
        up_g[features] = value[:, width:]
        return carry

    lax.fori_loop(0, D // tile, gate_step, 0)

    def down_step(i, carry):
        side, at = i // 2, lax.rem(i, 2)
        columns = pl.ds(pl.multiple_of(half + at * 512, 512), 512)
        down_g[:, pl.ds(pl.multiple_of(i * 512, 512), 512)] = dot(
            hid[...], rows_in[side, :, columns], (0, 0)
        )
        return carry

    lax.fori_loop(0, 4, down_step, 0)
    sent = (CHIPS - 1) * capacity
    wait_for(back.at[pl.ds(0, sent)], back_recv)
    normed_grad[...] = dot(select[...], back[...], (0, 0))
    wait_for(send.at[pl.ds(0, sent)], send_sem)
    wait_for(ret.at[pl.ds(0, sent)], back_send)
    for g in range(GROUPS):
        passing(g).wait_send()
        exchange(g).wait_send()


def experts(routes, weights, stream, gain, cot, gate_w, up_w, down_w):
    tokens, half = stream.shape
    slots = 2 * tokens * routes.shape[0]
    width = gate_w.shape[1]
    vmem = pl.BlockSpec(memory_space=pltpu.VMEM)
    hbm = pl.BlockSpec(memory_space=pl.ANY)
    f32, bf16 = jnp.float32, jnp.bfloat16
    dma = pltpu.SemaphoreType.DMA
    return pl.pallas_call(
        experts_kernel,
        out_shape=(
            jax.ShapeDtypeStruct((tokens, half), f32),
            jax.ShapeDtypeStruct((tokens, 128), f32),
            jax.ShapeDtypeStruct((D, width), f32),
            jax.ShapeDtypeStruct((D, width), f32),
            jax.ShapeDtypeStruct((width, D), f32),
        ),
        in_specs=[vmem] * 5 + [hbm] * 3,
        out_specs=(vmem,) * 5,
        scratch_shapes=[
            pltpu.VMEM((D, width), bf16),
            pltpu.VMEM((D, width), bf16),
            pltpu.VMEM((width, D), bf16),
            pltpu.VMEM((2, tokens, 128), f32),
            pltpu.VMEM((tokens, half), bf16),
            pltpu.VMEM((slots, tokens), bf16),
            pltpu.VMEM((slots, 2 * half), bf16),
            pltpu.VMEM((2, slots, 2 * half), bf16),
            pltpu.VMEM((slots, 2 * width), bf16),
            pltpu.VMEM((slots, width), bf16),
            pltpu.VMEM((slots, half), bf16),
            pltpu.VMEM((slots, half), bf16),
            pltpu.VMEM((slots, half), bf16),
            pltpu.VMEM((slots, half), bf16),
            pltpu.VMEM((slots, half), bf16),
            dma((3,)),
            dma((2,)),
            dma(()),
            dma((GROUPS,)),
            dma((GROUPS,)),
            dma((GROUPS,)),
            dma((GROUPS,)),
            dma((GROUPS,)),
            dma(()),
            dma(()),
        ],
        compiler_params=pltpu.CompilerParams(
            collective_id=0, has_side_effects=True, vmem_limit_bytes=60 << 20
        ),
        name="experts",
    )(routes, weights, stream, gain, cot, gate_w, up_w, down_w)


def tail_kernel(
    normed_grad,
    inverse_in,
    stream,
    gain,
    cot,
    value_in,
    out_gate,
    in_gate,
    taps,
    out_proj,
    stream_grad,
    proj_grad,
    input_grad,
    bgate_grad,
    cgate_grad,
    cross,
    whole,
    rim_in,
    rim_out,
    rim_back,
    conv,
    delta,
    shares,
    arrived,
    cross_sem,
    whole_sem,
    rim_sem,
    back_sem,
    share_sem,
):
    me, core = lax.axis_index("sp"), lax.axis_index("tp")
    partner = (me, 1 - core)
    tokens, half = stream.shape
    barrier = greet_all(me, core)
    stream_float = stream[...].astype(jnp.float32)
    part = jnp.sum(stream_float * gain[...] * normed_grad[...], axis=1, keepdims=True)
    cross[0] = jnp.broadcast_to(part, cross.shape[1:])
    pl.semaphore_wait(barrier, CHIPS)
    swap = remote(cross.at[0], cross.at[1], cross_sem.at[0], cross_sem.at[1], partner)
    swap.start()
    after, ahead = lax.rem(me + 1, CHIPS), lax.rem(me + CHIPS - 1, CHIPS)
    rims = [
        remote(
            ref.at[pl.ds(tokens - 16, 16)],
            rim_in.at[i],
            rim_sem.at[i],
            rim_sem.at[2 + i],
            (after, core),
        )
        for i, ref in enumerate((value_in, in_gate))
    ]
    for rim in rims:
        rim.start()
    swap.wait()
    inverse = inverse_in[:, 0:1]
    total = cross[0, :, 0:1] + cross[1, :, 0:1]
    grad = (
        cot[...].astype(jnp.float32)
        + inverse * gain[...] * normed_grad[...]
        - stream_float * inverse * inverse * inverse * total / D
    ).astype(jnp.bfloat16)
    stream_grad[...] = grad
    whole[core] = grad
    join = remote(
        whole.at[core], whole.at[core], whole_sem.at[0], whole_sem.at[1], partner
    )
    join.start()

    row = lax.broadcasted_iota(jnp.int32, conv.shape, 0)
    gated = in_gate[...].astype(jnp.float32) * value_in[...].astype(jnp.float32)
    for rim in rims:
        rim.wait()
    rim_gated = rim_in[1].astype(jnp.float32) * rim_in[0].astype(jnp.float32)
    rim_gated = jnp.where(me == 0, jnp.zeros_like(rim_gated), rim_gated)
    last, older = rim_gated[15:16], rim_gated[14:15]
    previous = jnp.where(row == 0, last, pltpu.roll(gated, 1, 0))
    before = jnp.where(row == 0, older, jnp.where(row == 1, last, pltpu.roll(gated, 2, 0)))
    conv[...] = taps[0:1] * before + taps[1:2] * previous + taps[2:3] * gated
    mixer_out = (out_gate[...].astype(jnp.float32) * conv[...]).astype(jnp.bfloat16)
    wait_for(whole.at[1 - core], whole_sem.at[1])
    mixer_grad = dot(whole[0], out_proj[:half]) + dot(whole[1], out_proj[half:])
    delta[...] = mixer_grad * out_gate[...].astype(jnp.float32)
    rim_out[...] = delta[0:8]
    give = remote(rim_out, rim_back, back_sem.at[0], back_sem.at[1], (ahead, core))
    for side in range(2):
        shares[side * half : (side + 1) * half] = dot(whole[side], mixer_out, (0, 0)).astype(
            jnp.bfloat16
        )
    give.start()
    height = proj_grad.shape[0]
    for j, k in enumerate(ORDER):
        peer = moved(me, k)
        remote(
            shares.at[pl.ds(pl.multiple_of(peer * height, height), height)],
            arrived.at[j],
            share_sem.at[0],
            share_sem.at[1],
            (peer, core),
        ).start()
    arrived[CHIPS - 1] = shares[pl.ds(pl.multiple_of(me * height, height), height)]
    bgate_grad[...] = (mixer_grad * conv[...]).astype(jnp.bfloat16)
    give.wait()
    rim_delta = jnp.where(me == CHIPS - 1, jnp.zeros_like(rim_back[...]), rim_back[...])
    nearest, second = rim_delta[0:1], rim_delta[1:2]
    here = delta[...]
    following = jnp.where(row == tokens - 1, nearest, pltpu.roll(here, tokens - 1, 0))
    beyond = jnp.where(
        row == tokens - 2,
        nearest,
        jnp.where(row == tokens - 1, second, pltpu.roll(here, tokens - 2, 0)),
    )
    gated_grad = taps[2:3] * here + taps[1:2] * following + taps[0:1] * beyond
    input_grad[...] = (gated_grad * in_gate[...].astype(jnp.float32)).astype(jnp.bfloat16)
    cgate_grad[...] = (gated_grad * value_in[...].astype(jnp.float32)).astype(jnp.bfloat16)
    wait_for(arrived.at[pl.ds(0, CHIPS - 1)], share_sem.at[1])
    total = arrived[0].astype(jnp.float32)
    for j in range(1, CHIPS):
        total = total + arrived[j].astype(jnp.float32)
    proj_grad[...] = total
    wait_for(shares.at[pl.ds(0, (CHIPS - 1) * height)], share_sem.at[0])
    wait_for(whole.at[core], whole_sem.at[0])


def tail(normed_grad, inverse, stream, gain, cot, value_in, out_gate, in_gate, taps, out_proj):
    tokens, half = stream.shape
    width = value_in.shape[1]
    height = D // CHIPS
    vmem = pl.BlockSpec(memory_space=pltpu.VMEM)
    f32, bf16 = jnp.float32, jnp.bfloat16
    dma = pltpu.SemaphoreType.DMA
    return pl.pallas_call(
        tail_kernel,
        out_shape=(
            jax.ShapeDtypeStruct((tokens, half), bf16),
            jax.ShapeDtypeStruct((height, width), f32),
            jax.ShapeDtypeStruct((tokens, width), bf16),
            jax.ShapeDtypeStruct((tokens, width), bf16),
            jax.ShapeDtypeStruct((tokens, width), bf16),
        ),
        in_specs=[vmem] * 10,
        out_specs=(vmem,) * 5,
        scratch_shapes=[
            pltpu.VMEM((2, tokens, 128), f32),
            pltpu.VMEM((2, tokens, half), bf16),
            pltpu.VMEM((2, 16, width), bf16),
            pltpu.VMEM((8, width), f32),
            pltpu.VMEM((8, width), f32),
            pltpu.VMEM((tokens, width), f32),
            pltpu.VMEM((tokens, width), f32),
            pltpu.VMEM((D, width), bf16),
            pltpu.VMEM((CHIPS, height, width), bf16),
            dma((2,)),
            dma((2,)),
            dma((4,)),
            dma((2,)),
            dma((2,)),
        ],
        compiler_params=pltpu.CompilerParams(
            collective_id=1, has_side_effects=True, vmem_limit_bytes=24 << 20
        ),
        name="tail",
    )(normed_grad, inverse, stream, gain, cot, value_in, out_gate, in_gate, taps, out_proj)


def local(
    stream,
    norm_gain,
    cotangent,
    route_weights,
    routes,
    conv_input,
    conv_bgate,
    conv_cgate,
    conv_taps,
    out_proj,
    gate_weight,
    up_weight,
    down_weight,
):
    gain = norm_gain[None, :]
    normed_grad, inverse, gate_g, up_g, down_g = experts(
        routes.T,
        route_weights.T,
        stream,
        gain,
        cotangent,
        gate_weight[0],
        up_weight[0],
        down_weight[0],
    )
    stream_grad, proj_grad, input_grad, bgate_grad, cgate_grad = tail(
        normed_grad,
        inverse,
        stream,
        gain,
        cotangent,
        conv_input,
        conv_bgate,
        conv_cgate,
        conv_taps,
        out_proj,
    )
    return (
        stream_grad,
        proj_grad,
        input_grad,
        bgate_grad,
        cgate_grad,
        gate_g[None],
        up_g[None],
        down_g[None],
    )


def solution(mesh):
    return jax.shard_map(
        local,
        mesh=mesh,
        in_specs=(
            P("sp", "tp"),
            P("tp"),
            P("sp", "tp"),
            P("sp", None),
            P("sp", None),
            P("sp", "tp"),
            P("sp", "tp"),
            P("sp", "tp"),
            P(None, "tp"),
            P(None, "tp"),
            P("sp", None, "tp"),
            P("sp", None, "tp"),
            P("sp", "tp", None),
        ),
        out_specs=(
            P("sp", "tp"),
            P("sp", "tp"),
            P("sp", "tp"),
            P("sp", "tp"),
            P("sp", "tp"),
            P("sp", None, "tp"),
            P("sp", None, "tp"),
            P("sp", "tp", None),
        ),
        check_vma=False,
    )
```

```python
import functools

import jax
import jax.numpy as jnp
from jax import lax
from jax.experimental import pallas as pl
from jax.experimental.pallas import tpu as pltpu
from jax.sharding import PartitionSpec as P

D = 2048
EPSILON = 1e-06
MESH = pl.DeviceIdType.MESH
SIDE = 4
CHIPS = SIDE**3


def _parts(k):
    return k // 16, (k // 4) % 4, k % 4


def _join(z, y, x):
    return (z % 4) * 16 + (y % 4) * 4 + x % 4


def _shift_order():
    hops = lambda k: sum(min(a, SIDE - a) for a in _parts(k))
    turn = lambda k: _join(*(_parts(k)[1:] + _parts(k)[:1]))
    back = lambda k: _join(*(-a for a in _parts(k)))
    order = []
    for k in sorted(range(1, CHIPS), key=lambda k: -hops(k)):
        for kk in (k, turn(k), turn(turn(k))):
            for other in (kk,):
                if other not in order:
                    order.append(other)
        for kk in (k, turn(k), turn(turn(k))):
            if back(kk) not in order:
                order.append(back(kk))
    return order


ORDER = _shift_order()


def moved(me, k, sign=1):
    z, y, x = me // 16, lax.rem(me // 4, 4), lax.rem(me, 4)
    kz, ky, kx = (a if sign > 0 else (SIDE - a) % SIDE for a in _parts(k))
    return lax.rem(z + kz, 4) * 16 + lax.rem(y + ky, 4) * 4 + lax.rem(x + kx, 4)


GROUPS = 8
BLOCKS = CHIPS // GROUPS
UNITS = 8
FIRST = (0, 0, 0, 1, 1, 1, 2, 2)
UNIT_ORDER = (0, 3, 6, 1, 4, 7, 2, 5)
PLANE = tuple(
    sorted(
        ((i, j) for i in range(SIDE) for j in range(SIDE) if i or j),
        key=lambda p: -sum(min(a, SIDE - a) for a in p),
    )
)


def greet_all(me, core):
    barrier = pltpu.get_barrier_semaphore()
    for k in ORDER:
        pl.semaphore_signal(
            barrier, inc=1, device_id=(moved(me, k), core), device_id_type=MESH
        )
    pl.semaphore_signal(barrier, inc=1, device_id=(me, 1 - core), device_id_type=MESH)
    return barrier


def remote(source, target, send_sem, recv_sem, peer):
    return pltpu.make_async_remote_copy(
        src_ref=source,
        dst_ref=target,
        send_sem=send_sem,
        recv_sem=recv_sem,
        device_id=peer,
        device_id_type=MESH,
    )


def wait_for(ref, sem):
    pltpu.make_async_copy(ref, ref, sem).wait()


def dot(left, right, over=(1, 0)):
    return lax.dot_general(
        left, right, (((over[0],), (over[1],)), ((), ())), preferred_element_type=jnp.float32
    )


def experts_kernel(
    routes_hbm,
    weights_hbm,
    stream_hbm,
    gain_hbm,
    cot_hbm,
    gate_hbm,
    up_hbm,
    down_hbm,
    normed_grad,
    inverse_out,
    gate_g,
    up_g,
    down_g,
    routes,
    weights,
    stream,
    gain,
    cot,
    gate_w,
    up_w,
    down_w,
    square,
    select,
    send,
    rows_in,
    pre,
    hid,
    theirs,
    mine,
    other,
    back,
    load_sem,
    square_sem,
    send_sem,
    recv_sem,
    pass_send,
    pass_recv,
    part_send,
    part_recv,
    back_send,
    back_recv,
):
    me, core = lax.axis_index("sp"), lax.axis_index("tp")
    partner = (me, 1 - core)
    capacity = send.shape[0] // CHIPS
    half = stream.shape[1]
    depth = BLOCKS * capacity
    width = gate_w.shape[1]
    pairs = (
        (stream_hbm, stream),
        (gain_hbm, gain),
        (routes_hbm, routes),
        (weights_hbm, weights),
        (cot_hbm, cot),
        (gate_hbm, gate_w),
        (up_hbm, up_w),
        (down_hbm, down_w),
    )
    loads = [pltpu.make_async_copy(a, b, load_sem.at[i]) for i, (a, b) in enumerate(pairs)]
    for load in loads:
        load.start()
    barrier = greet_all(me, core)
    for load in loads[:5]:
        load.wait()
    stream_float = stream[...].astype(jnp.float32)
    part = jnp.sum(stream_float * stream_float, axis=1, keepdims=True)
    square[0] = jnp.broadcast_to(part, square.shape[1:])
    pl.semaphore_wait(barrier, CHIPS)
    swap = remote(square.at[0], square.at[1], square_sem.at[0], square_sem.at[1], partner)
    swap.start()

    tokens = stream.shape[0]
    first, second = routes[0:1, :], routes[1:2, :]
    expert = lax.broadcasted_iota(jnp.int32, (CHIPS, tokens), 0)
    on_first, on_second = expert == first, expert == second
    named = jnp.where(on_first | on_second, 1.0, 0.0).astype(jnp.bfloat16)
    before = lax.broadcasted_iota(jnp.int32, (tokens, tokens), 0) < lax.broadcasted_iota(
        jnp.int32, (tokens, tokens), 1
    )
    earlier = dot(named, jnp.where(before, 1.0, 0.0).astype(jnp.bfloat16))

    def target_of(on, route):
        rank = jnp.sum(jnp.where(on, earlier, 0.0), axis=0, keepdims=True)
        return route * capacity + rank.astype(jnp.int32)

    first_target, second_target = target_of(on_first, first), target_of(on_second, second)
    chunk = 256
    slot_weights = []
    for at in range(0, CHIPS * capacity, chunk):
        place = lax.broadcasted_iota(jnp.int32, (chunk, tokens), 0) + at
        is_first, is_second = place == first_target, place == second_target
        select[at : at + chunk] = jnp.where(is_first | is_second, 1.0, 0.0).astype(jnp.bfloat16)
        slot_weights.append(
            jnp.sum(
                jnp.where(is_first, weights[0:1, :], 0.0)
                + jnp.where(is_second, weights[1:2, :], 0.0),
                axis=1,
                keepdims=True,
            )
        )
    swap.wait()
    inverse = lax.rsqrt((square[0, :, 0:1] + square[1, :, 0:1]) / D + EPSILON)
    inverse_out[...] = jnp.broadcast_to(inverse, inverse_out.shape)
    normed = mine.at[pl.ds(0, tokens)]
    normed[...] = (stream_float * inverse * gain[...]).astype(jnp.bfloat16)
    for i, at in enumerate(range(0, CHIPS * capacity, chunk)):
        chosen = select[at : at + chunk]
        send[at : at + chunk, :half] = dot(chosen, normed[...]).astype(jnp.bfloat16)
        send[at : at + chunk, half:] = (slot_weights[i] * dot(chosen, cot[...])).astype(
            jnp.bfloat16
        )

    def block(index):
        return pl.ds(pl.multiple_of(index * capacity, capacity), capacity)

    for j, k in enumerate(ORDER):
        peer = moved(me, k)
        remote(
            send.at[block(peer)],
            rows_in.at[core, pl.ds(j * capacity, capacity)],
            send_sem,
            recv_sem.at[j // BLOCKS],
            (peer, core),
        ).start()
    rows_in[core, (CHIPS - 1) * capacity :] = send[block(me)]
    for load in loads[5:]:
        load.wait()

    def group(g, count=depth):
        return pl.ds(pl.multiple_of(g * depth, depth), count)

    def passing(g):
        piece = rows_in.at[core, group(g)]
        return remote(piece, piece, pass_send.at[g], pass_recv.at[g], partner)

    def exchange(g):
        return remote(
            theirs.at[group(lax.rem(g, 2))], other.at[group(g)], part_send.at[g], part_recv.at[g], partner
        )

    def take(g):
        @pl.when(g < GROUPS - 1)
        def _():
            wait_for(rows_in.at[core, group(g)], recv_sem.at[g])

        @pl.when(g == GROUPS - 1)
        def _():
            wait_for(rows_in.at[core, group(g, depth - capacity)], recv_sem.at[g])

        passing(g).start()

    def compute(g):
        wait_for(rows_in.at[1 - core, group(g)], pass_recv.at[g])
        rows = group(g)
        gate_lin = dot(rows_in[0, rows, :half], gate_w[:half]) + dot(
            rows_in[1, rows, :half], gate_w[half:]
        )
        up_lin = dot(rows_in[0, rows, :half], up_w[:half]) + dot(
            rows_in[1, rows, :half], up_w[half:]
        )
        hidden_grad = dot(rows_in[0, rows, half:], down_w[:, :half], (1, 1)) + dot(
            rows_in[1, rows, half:], down_w[:, half:], (1, 1)
        )
        sigmoid_gate = jax.nn.sigmoid(gate_lin)
        silu_gate = gate_lin * sigmoid_gate
        hid[rows] = (silu_gate * up_lin).astype(jnp.bfloat16)
        gate_pre = (
            hidden_grad * up_lin * sigmoid_gate * (1.0 + gate_lin * (1.0 - sigmoid_gate))
        ).astype(jnp.bfloat16)
        up_pre = (hidden_grad * silu_gate).astype(jnp.bfloat16)
        pre[rows, :width] = gate_pre
        pre[rows, width:] = up_pre
        pl.when(g >= 2)(lambda: exchange(g - 2).wait_send())
        for target, at, side in (
            (theirs, group(lax.rem(g, 2)), 1 - core),
            (mine, rows, core),
        ):
            features = pl.ds(pl.multiple_of(side * half, half), half)
            value = dot(gate_pre, gate_w[features], (1, 1)) + dot(up_pre, up_w[features], (1, 1))
            target[at] = value.astype(jnp.bfloat16)
        exchange(g).start()

    def finish(g):
        wait_for(other.at[group(g)], part_recv.at[g])
        rows = group(g)
        mine[rows] = (mine[rows].astype(jnp.float32) + other[rows].astype(jnp.float32)).astype(
            jnp.bfloat16
        )
        for i in range(BLOCKS):
            k = jnp.int32(ORDER[i])
            for later in range(1, GROUPS):
                if later * BLOCKS + i < CHIPS - 1:
                    k = jnp.where(g == later, ORDER[later * BLOCKS + i], k)
            z = lax.rem(me // 16 + 4 - k // 16, 4)
            y = lax.rem(lax.rem(me // 4, 4) + 4 - lax.rem(k // 4, 4), 4)
            x = lax.rem(lax.rem(me, 4) + 4 - lax.rem(k, 4), 4)
            go = remote(
                mine.at[block(g * BLOCKS + i)],
                back.at[block(me)],
                back_send,
                back_recv,
                (z * 16 + y * 4 + x, core),
            )
            if i < BLOCKS - 1:
                go.start()
            else:
                pl.when(g < GROUPS - 1)(go.start)

    def step(i, carry):
        pl.when(i < GROUPS)(lambda: take(i))
        pl.when((i >= 1) & (i <= GROUPS))(lambda: compute(i - 1))
        pl.when(i >= 2)(lambda: finish(i - 2))
        return carry

    lax.fori_loop(0, GROUPS + 2, step, 0)
    back[block(me)] = mine[(CHIPS - 1) * capacity :]

    tile = 128

    def gate_step(i, carry):
        side, at = i // (half // tile), lax.rem(i, half // tile)
        columns = pl.ds(pl.multiple_of(at * tile, tile), tile)
        value = dot(rows_in[side, :, columns], pre[...], (0, 0))
        features = pl.ds(pl.multiple_of(i * tile, tile), tile)
        gate_g[features] = value[:, :width]
        up_g[features] = value[:, width:]
        return carry

    lax.fori_loop(0, D // tile, gate_step, 0)

    def down_step(i, carry):
        side, at = i // 2, lax.rem(i, 2)
        columns = pl.ds(pl.multiple_of(half + at * 512, 512), 512)
        down_g[:, pl.ds(pl.multiple_of(i * 512, 512), 512)] = dot(
            hid[...], rows_in[side, :, columns], (0, 0)
        )
        return carry

    lax.fori_loop(0, 4, down_step, 0)
    sent = (CHIPS - 1) * capacity
    wait_for(back.at[pl.ds(0, sent)], back_recv)
    normed_grad[...] = dot(select[...], back[...], (0, 0))
    wait_for(send.at[pl.ds(0, sent)], send_sem)
    wait_for(mine.at[pl.ds(0, sent)], back_send)
    for g in range(GROUPS):
        passing(g).wait_send()
    for g in range(GROUPS - 2, GROUPS):
        exchange(g).wait_send()


def experts(routes, weights, stream, gain, cot, gate_w, up_w, down_w):
    tokens, half = stream.shape
    slots = 2 * tokens * routes.shape[0]
    width = gate_w.shape[1]
    vmem = pl.BlockSpec(memory_space=pltpu.VMEM)
    hbm = pl.BlockSpec(memory_space=pltpu.HBM)
    f32, bf16 = jnp.float32, jnp.bfloat16
    dma = pltpu.SemaphoreType.DMA
    return pl.pallas_call(
        experts_kernel,
        out_shape=(
            jax.ShapeDtypeStruct((tokens, half), f32),
            jax.ShapeDtypeStruct((tokens, 128), f32),
            jax.ShapeDtypeStruct((D, width), f32),
            jax.ShapeDtypeStruct((D, width), f32),
            jax.ShapeDtypeStruct((width, D), f32),
        ),
        in_specs=[hbm] * 8,
        out_specs=(vmem,) * 5,
        scratch_shapes=[
            pltpu.VMEM(routes.shape, jnp.int32),
            pltpu.VMEM(weights.shape, f32),
            pltpu.VMEM((tokens, half), bf16),
            pltpu.VMEM((1, half), f32),
            pltpu.VMEM((tokens, half), bf16),
            pltpu.VMEM((D, width), bf16),
            pltpu.VMEM((D, width), bf16),
            pltpu.VMEM((width, D), bf16),
            pltpu.VMEM((2, tokens, 128), f32),
            pltpu.VMEM((slots, tokens), bf16),
            pltpu.VMEM((slots, 2 * half), bf16),
            pltpu.VMEM((2, slots, 2 * half), bf16),
            pltpu.VMEM((slots, 2 * width), bf16),
            pltpu.VMEM((slots, width), bf16),
            pltpu.VMEM((2 * slots // GROUPS, half), bf16),
            pltpu.VMEM((slots, half), bf16),
            pltpu.VMEM((slots, half), bf16),
            pltpu.VMEM((slots, half), bf16),
            dma((8,)),
            dma((2,)),
            dma(()),
            dma((GROUPS,)),
            dma((GROUPS,)),
            dma((GROUPS,)),
            dma((GROUPS,)),
            dma((GROUPS,)),
            dma(()),
            dma(()),
        ],
        compiler_params=pltpu.CompilerParams(
            collective_id=0, has_side_effects=True, vmem_limit_bytes=32 << 20
        ),
        name="experts",
    )(
        *(
            pltpu.with_memory_space_constraint(a, pltpu.HBM)
            for a in (routes, weights, stream, gain, cot, gate_w, up_w, down_w)
        )
    )


def tail_kernel(
    normed_grad,
    inverse_in,
    stream,
    gain,
    cot,
    value_in,
    out_gate,
    in_gate,
    taps,
    out_proj,
    stream_grad,
    proj_grad,
    input_grad,
    bgate_grad,
    cgate_grad,
    cross,
    whole,
    rim_in,
    rim_out,
    rim_back,
    conv,
    delta,
    shares,
    got,
    half_sum,
    final,
    cross_sem,
    whole_sem,
    rim_sem,
    back_sem,
    share_send,
    share_recv,
    sum_send,
    sum_recv,
):
    me, core = lax.axis_index("sp"), lax.axis_index("tp")
    partner = (me, 1 - core)
    tokens, half = stream.shape
    barrier = greet_all(me, core)
    stream_float = stream[...].astype(jnp.float32)
    part = jnp.sum(stream_float * gain[...] * normed_grad[...], axis=1, keepdims=True)
    cross[0] = jnp.broadcast_to(part, cross.shape[1:])
    pl.semaphore_wait(barrier, CHIPS)
    swap = remote(cross.at[0], cross.at[1], cross_sem.at[0], cross_sem.at[1], partner)
    swap.start()
    after, ahead = lax.rem(me + 1, CHIPS), lax.rem(me + CHIPS - 1, CHIPS)
    rims = [
        remote(
            ref.at[pl.ds(tokens - 16, 16)],
            rim_in.at[i],
            rim_sem.at[i],
            rim_sem.at[2 + i],
            (after, core),
        )
        for i, ref in enumerate((value_in, in_gate))
    ]
    for rim in rims:
        rim.start()
    swap.wait()
    inverse = inverse_in[:, 0:1]
    total = cross[0, :, 0:1] + cross[1, :, 0:1]
    grad = (
        cot[...].astype(jnp.float32)
        + inverse * gain[...] * normed_grad[...]
        - stream_float * inverse * inverse * inverse * total / D
    ).astype(jnp.bfloat16)
    stream_grad[...] = grad
    whole[core] = grad
    join = remote(
        whole.at[core], whole.at[core], whole_sem.at[0], whole_sem.at[1], partner
    )
    join.start()

    row = lax.broadcasted_iota(jnp.int32, conv.shape, 0)
    gated = in_gate[...].astype(jnp.float32) * value_in[...].astype(jnp.float32)
    for rim in rims:
        rim.wait()
    rim_gated = rim_in[1].astype(jnp.float32) * rim_in[0].astype(jnp.float32)
    rim_gated = jnp.where(me == 0, jnp.zeros_like(rim_gated), rim_gated)
    last, older = rim_gated[15:16], rim_gated[14:15]
    previous = jnp.where(row == 0, last, pltpu.roll(gated, 1, 0))
    before = jnp.where(row == 0, older, jnp.where(row == 1, last, pltpu.roll(gated, 2, 0)))
    conv[...] = taps[0:1] * before + taps[1:2] * previous + taps[2:3] * gated
    mixer_out = (out_gate[...].astype(jnp.float32) * conv[...]).astype(jnp.bfloat16)

    def split(side):
        value = dot(whole[side], mixer_out, (0, 0)).astype(jnp.bfloat16)
        value = value.reshape(2, SIDE, SIDE, 2, 16, value.shape[1])
        for u in range(UNITS):
            r, c = u // 4, u % 4
            shares[u, pl.ds(side * 2, 2)] = value[:, :, :, r, :, c * 128 : (c + 1) * 128]

    split(core)
    wait_for(whole.at[1 - core], whole_sem.at[1])
    split(1 - core)
    here = (me // 16, lax.rem(me // 4, 4), lax.rem(me, 4))

    def at_place(place):
        return (place[0] * 16 + place[1] * 4 + place[2], core)

    def shifted(moves):
        return [lax.rem(h + m, 4) for h, m in zip(here, moves)]

    def plane(u, index):
        first = FIRST[u]
        return shares.at[(u,) + (slice(None),) * first + (index,)]

    for u in UNIT_ORDER:
        for i, step in enumerate((2, 1, 3)):
            place = shifted([step if d == FIRST[u] else 0 for d in range(3)])
            remote(
                plane(u, place[FIRST[u]]),
                got.at[u, i],
                share_send,
                share_recv.at[u],
                at_place(place),
            ).start()
    mixer_grad = dot(whole[0], out_proj[:half]) + dot(whole[1], out_proj[half:])
    delta[...] = mixer_grad * out_gate[...].astype(jnp.float32)
    rim_out[...] = delta[0:8]
    give = remote(rim_out, rim_back, back_sem.at[0], back_sem.at[1], (ahead, core))
    bgate_grad[...] = (mixer_grad * conv[...]).astype(jnp.bfloat16)
    give.start()

    def spread(u):
        rest = [d for d in range(3) if d != FIRST[u]]
        for i, (one, two) in enumerate(PLANE):
            moves = [0, 0, 0]
            moves[rest[0]], moves[rest[1]] = one, two
            place = shifted(moves)
            remote(
                half_sum.at[u, place[rest[0]], place[rest[1]]],
                final.at[u, i],
                sum_send,
                sum_recv.at[u],
                at_place(place),
            ).start()

    earlier = None
    for u in UNIT_ORDER:
        wait_for(got.at[u], share_recv.at[u])
        value = plane(u, here[FIRST[u]])[...].astype(jnp.float32)
        for i in range(SIDE - 1):
            value = value + got[u, i].astype(jnp.float32)
        half_sum[u] = value
        if earlier is not None:
            spread(earlier)
        earlier = u
    spread(earlier)
    give.wait()
    rim_delta = jnp.where(me == CHIPS - 1, jnp.zeros_like(rim_back[...]), rim_back[...])
    nearest, second = rim_delta[0:1], rim_delta[1:2]
    change = delta[...]
    following = jnp.where(row == tokens - 1, nearest, pltpu.roll(change, tokens - 1, 0))
    beyond = jnp.where(
        row == tokens - 2,
        nearest,
        jnp.where(row == tokens - 1, second, pltpu.roll(change, tokens - 2, 0)),
    )
    gated_grad = taps[2:3] * change + taps[1:2] * following + taps[0:1] * beyond
    input_grad[...] = (gated_grad * in_gate[...].astype(jnp.float32)).astype(jnp.bfloat16)
    cgate_grad[...] = (gated_grad * value_in[...].astype(jnp.float32)).astype(jnp.bfloat16)
    for u in UNIT_ORDER:
        rest = [d for d in range(3) if d != FIRST[u]]
        wait_for(final.at[u], sum_recv.at[u])
        total = half_sum[u, here[rest[0]], here[rest[1]]]
        for i in range(len(PLANE)):
            total = total + final[u, i]
        r, c = u // 4, u % 4
        proj_grad[r * 16 : (r + 1) * 16, c * 128 : (c + 1) * 128] = total
    wait_for(got, share_send)
    wait_for(final, sum_send)
    wait_for(whole.at[core], whole_sem.at[0])


def tail(normed_grad, inverse, stream, gain, cot, value_in, out_gate, in_gate, taps, out_proj):
    tokens, half = stream.shape
    width = value_in.shape[1]
    height = D // CHIPS
    vmem = pl.BlockSpec(memory_space=pltpu.VMEM)
    f32, bf16 = jnp.float32, jnp.bfloat16
    dma = pltpu.SemaphoreType.DMA
    return pl.pallas_call(
        tail_kernel,
        out_shape=(
            jax.ShapeDtypeStruct((tokens, half), bf16),
            jax.ShapeDtypeStruct((height, width), f32),
            jax.ShapeDtypeStruct((tokens, width), bf16),
            jax.ShapeDtypeStruct((tokens, width), bf16),
            jax.ShapeDtypeStruct((tokens, width), bf16),
        ),
        in_specs=[vmem] * 10,
        out_specs=(vmem,) * 5,
        scratch_shapes=[
            pltpu.VMEM((2, tokens, 128), f32),
            pltpu.VMEM((2, tokens, half), bf16),
            pltpu.VMEM((2, 16, width), bf16),
            pltpu.VMEM((8, width), f32),
            pltpu.VMEM((8, width), f32),
            pltpu.VMEM((tokens, width), f32),
            pltpu.VMEM((tokens, width), f32),
            pltpu.VMEM((UNITS, SIDE, SIDE, SIDE, 16, 128), bf16),
            pltpu.VMEM((UNITS, SIDE - 1, SIDE, SIDE, 16, 128), bf16),
            pltpu.VMEM((UNITS, SIDE, SIDE, 16, 128), f32),
            pltpu.VMEM((UNITS, len(PLANE), 16, 128), f32),
            dma((2,)),
            dma((2,)),
            dma((4,)),
            dma((2,)),
            dma(()),
            dma((UNITS,)),
            dma(()),
            dma((UNITS,)),
        ],
        compiler_params=pltpu.CompilerParams(
            collective_id=1, has_side_effects=True, vmem_limit_bytes=12 << 20
        ),
        name="tail",
    )(normed_grad, inverse, stream, gain, cot, value_in, out_gate, in_gate, taps, out_proj)


def store_kernel(*refs):
    count = len(refs) // 2
    sem = refs[-1]
    copies = [
        pltpu.make_async_copy(refs[i], refs[count + i], sem.at[i]) for i in range(count)
    ]
    for copy in copies:
        copy.start()
    for copy in copies:
        copy.wait()


def store(*arrays):
    return pl.pallas_call(
        store_kernel,
        out_shape=tuple(jax.ShapeDtypeStruct(a.shape, a.dtype) for a in arrays),
        in_specs=[pl.BlockSpec(memory_space=pltpu.VMEM)] * len(arrays),
        out_specs=(pl.BlockSpec(memory_space=pltpu.HBM),) * len(arrays),
        scratch_shapes=[pltpu.SemaphoreType.DMA((len(arrays),))],
        compiler_params=pltpu.CompilerParams(vmem_limit_bytes=1 << 20),
        name="store",
    )(*arrays)


def local(
    stream,
    norm_gain,
    cotangent,
    route_weights,
    routes,
    conv_input,
    conv_bgate,
    conv_cgate,
    conv_taps,
    out_proj,
    gate_weight,
    up_weight,
    down_weight,
):
    gain = norm_gain[None, :]
    normed_grad, inverse, gate_g, up_g, down_g = experts(
        routes.T,
        route_weights.T,
        stream,
        gain,
        cotangent,
        gate_weight[0],
        up_weight[0],
        down_weight[0],
    )
    stream_grad, proj_grad, input_grad, bgate_grad, cgate_grad = tail(
        normed_grad,
        inverse,
        stream,
        gain,
        cotangent,
        conv_input,
        conv_bgate,
        conv_cgate,
        conv_taps,
        out_proj,
    )
    outs = store(
        stream_grad, proj_grad, input_grad, bgate_grad, cgate_grad, gate_g, up_g, down_g
    )
    return (*outs[:5], *(out[None] for out in outs[5:]))


def solution(mesh):
    return jax.shard_map(
        local,
        mesh=mesh,
        in_specs=(
            P("sp", "tp"),
            P("tp"),
            P("sp", "tp"),
            P("sp", None),
            P("sp", None),
            P("sp", "tp"),
            P("sp", "tp"),
            P("sp", "tp"),
            P(None, "tp"),
            P(None, "tp"),
            P("sp", None, "tp"),
            P("sp", None, "tp"),
            P("sp", "tp", None),
        ),
        out_specs=(
            P("sp", "tp"),
            P("sp", "tp"),
            P("sp", "tp"),
            P("sp", "tp"),
            P("sp", "tp"),
            P("sp", None, "tp"),
            P("sp", None, "tp"),
            P("sp", "tp", None),
        ),
        check_vma=False,
    )
```

```python
import functools

import jax
import jax.numpy as jnp
from jax import lax
from jax.experimental import pallas as pl
from jax.experimental.pallas import tpu as pltpu
from jax.sharding import PartitionSpec as P

D = 2048
EPSILON = 1e-06
MESH = pl.DeviceIdType.MESH
SIDE = 4
CHIPS = SIDE**3


def _parts(k):
    return k // 16, (k // 4) % 4, k % 4


def _join(z, y, x):
    return (z % 4) * 16 + (y % 4) * 4 + x % 4


def _shift_order():
    hops = lambda k: sum(min(a, SIDE - a) for a in _parts(k))
    turn = lambda k: _join(*(_parts(k)[1:] + _parts(k)[:1]))
    back = lambda k: _join(*(-a for a in _parts(k)))
    order = []
    for k in sorted(range(1, CHIPS), key=lambda k: -hops(k)):
        for kk in (k, turn(k), turn(turn(k))):
            for other in (kk,):
                if other not in order:
                    order.append(other)
        for kk in (k, turn(k), turn(turn(k))):
            if back(kk) not in order:
                order.append(back(kk))
    return order


ORDER = _shift_order()


def moved(me, k, sign=1):
    z, y, x = me // 16, lax.rem(me // 4, 4), lax.rem(me, 4)
    kz, ky, kx = (a if sign > 0 else (SIDE - a) % SIDE for a in _parts(k))
    return lax.rem(z + kz, 4) * 16 + lax.rem(y + ky, 4) * 4 + lax.rem(x + kx, 4)


GROUPS = 8
BLOCKS = CHIPS // GROUPS
UNITS = 8
FIRST = (0, 0, 0, 1, 1, 1, 2, 2)
UNIT_ORDER = (0, 3, 6, 1, 4, 7, 2, 5)
PLANE = tuple(
    sorted(
        ((i, j) for i in range(SIDE) for j in range(SIDE) if i or j),
        key=lambda p: -sum(min(a, SIDE - a) for a in p),
    )
)


def greet_all(me, core):
    barrier = pltpu.get_barrier_semaphore()
    for k in ORDER:
        pl.semaphore_signal(
            barrier, inc=1, device_id=(moved(me, k), core), device_id_type=MESH
        )
    pl.semaphore_signal(barrier, inc=1, device_id=(me, 1 - core), device_id_type=MESH)
    return barrier


def remote(source, target, send_sem, recv_sem, peer):
    return pltpu.make_async_remote_copy(
        src_ref=source,
        dst_ref=target,
        send_sem=send_sem,
        recv_sem=recv_sem,
        device_id=peer,
        device_id_type=MESH,
    )


def wait_for(ref, sem):
    pltpu.make_async_copy(ref, ref, sem).wait()


def dot(left, right, over=(1, 0)):
    return lax.dot_general(
        left, right, (((over[0],), (over[1],)), ((), ())), preferred_element_type=jnp.float32
    )


def experts_kernel(
    routes_hbm,
    weights_hbm,
    stream_hbm,
    gain_hbm,
    cot_hbm,
    gate_hbm,
    up_hbm,
    down_hbm,
    normed_grad,
    inverse_out,
    gate_g,
    up_g,
    down_g,
    routes,
    weights,
    stream,
    gain,
    cot,
    gate_w,
    up_w,
    down_w,
    square,
    select,
    send,
    rows_in,
    pre,
    hid,
    theirs,
    mine,
    other,
    back,
    load_sem,
    square_sem,
    send_sem,
    recv_sem,
    pass_send,
    pass_recv,
    part_send,
    part_recv,
    back_send,
    back_recv,
):
    me, core = lax.axis_index("sp"), lax.axis_index("tp")
    partner = (me, 1 - core)
    capacity = send.shape[0] // CHIPS
    half = stream.shape[1]
    depth = BLOCKS * capacity
    width = gate_w.shape[1]
    pairs = (
        (stream_hbm, stream),
        (gain_hbm, gain),
        (routes_hbm, routes),
        (weights_hbm, weights),
        (cot_hbm, cot),
        (gate_hbm, gate_w),
        (up_hbm, up_w),
        (down_hbm, down_w),
    )
    loads = [pltpu.make_async_copy(a, b, load_sem.at[i]) for i, (a, b) in enumerate(pairs)]
    for load in loads:
        load.start()
    barrier = greet_all(me, core)
    for load in loads[:5]:
        load.wait()
    stream_float = stream[...].astype(jnp.float32)
    part = jnp.sum(stream_float * stream_float, axis=1, keepdims=True)
    square[0] = jnp.broadcast_to(part, square.shape[1:])
    pl.semaphore_wait(barrier, CHIPS)
    swap = remote(square.at[0], square.at[1], square_sem.at[0], square_sem.at[1], partner)
    swap.start()

    tokens = stream.shape[0]
    first, second = routes[0:1, :], routes[1:2, :]
    expert = lax.broadcasted_iota(jnp.int32, (CHIPS, tokens), 0)
    on_first, on_second = expert == first, expert == second
    named = jnp.where(on_first | on_second, 1.0, 0.0).astype(jnp.bfloat16)
    before = lax.broadcasted_iota(jnp.int32, (tokens, tokens), 0) < lax.broadcasted_iota(
        jnp.int32, (tokens, tokens), 1
    )
    earlier = dot(named, jnp.where(before, 1.0, 0.0).astype(jnp.bfloat16))

    def target_of(on, route):
        rank = jnp.sum(jnp.where(on, earlier, 0.0), axis=0, keepdims=True)
        return route * capacity + rank.astype(jnp.int32)

    first_target, second_target = target_of(on_first, first), target_of(on_second, second)
    chunk = 256
    slot_weights = []
    for at in range(0, CHIPS * capacity, chunk):
        place = lax.broadcasted_iota(jnp.int32, (chunk, tokens), 0) + at
        is_first, is_second = place == first_target, place == second_target
        select[at : at + chunk] = jnp.where(is_first | is_second, 1.0, 0.0).astype(jnp.bfloat16)
        slot_weights.append(
            jnp.sum(
                jnp.where(is_first, weights[0:1, :], 0.0)
                + jnp.where(is_second, weights[1:2, :], 0.0),
                axis=1,
                keepdims=True,
            )
        )
    swap.wait()
    inverse = lax.rsqrt((square[0, :, 0:1] + square[1, :, 0:1]) / D + EPSILON)
    inverse_out[...] = jnp.broadcast_to(inverse, inverse_out.shape)
    normed = mine.at[pl.ds(0, tokens)]
    normed[...] = (stream_float * inverse * gain[...]).astype(jnp.bfloat16)
    for i, at in enumerate(range(0, CHIPS * capacity, chunk)):
        chosen = select[at : at + chunk]
        send[at : at + chunk, :half] = dot(chosen, normed[...]).astype(jnp.bfloat16)
        send[at : at + chunk, half:] = (slot_weights[i] * dot(chosen, cot[...])).astype(
            jnp.bfloat16
        )

    def block(index):
        return pl.ds(pl.multiple_of(index * capacity, capacity), capacity)

    for i, k in enumerate(ORDER):
        opposite = _join(*(-a for a in _parts(k)))
        j = jnp.where(core == 0, i, ORDER.index(opposite))
        peer = jnp.where(core == 0, moved(me, k), moved(me, opposite))
        remote(
            send.at[block(peer)],
            rows_in.at[core, block(j)],
            send_sem,
            recv_sem.at[j // BLOCKS],
            (peer, core),
        ).start()
    rows_in[core, (CHIPS - 1) * capacity :] = send[block(me)]
    for load in loads[5:]:
        load.wait()

    def group(g, count=depth):
        return pl.ds(pl.multiple_of(g * depth, depth), count)

    def passing(g):
        piece = rows_in.at[core, group(g)]
        return remote(piece, piece, pass_send.at[g], pass_recv.at[g], partner)

    def exchange(g):
        return remote(
            theirs.at[group(lax.rem(g, 2))], other.at[group(g)], part_send.at[g], part_recv.at[g], partner
        )

    def take(g):
        @pl.when(g < GROUPS - 1)
        def _():
            wait_for(rows_in.at[core, group(g)], recv_sem.at[g])

        @pl.when(g == GROUPS - 1)
        def _():
            wait_for(rows_in.at[core, group(g, depth - capacity)], recv_sem.at[g])

        passing(g).start()

    def compute(g):
        wait_for(rows_in.at[1 - core, group(g)], pass_recv.at[g])
        rows = group(g)
        gate_lin = dot(rows_in[0, rows, :half], gate_w[:half]) + dot(
            rows_in[1, rows, :half], gate_w[half:]
        )
        up_lin = dot(rows_in[0, rows, :half], up_w[:half]) + dot(
            rows_in[1, rows, :half], up_w[half:]
        )
        hidden_grad = dot(rows_in[0, rows, half:], down_w[:, :half], (1, 1)) + dot(
            rows_in[1, rows, half:], down_w[:, half:], (1, 1)
        )
        sigmoid_gate = jax.nn.sigmoid(gate_lin)
        silu_gate = gate_lin * sigmoid_gate
        hid[rows] = (silu_gate * up_lin).astype(jnp.bfloat16)
        gate_pre = (
            hidden_grad * up_lin * sigmoid_gate * (1.0 + gate_lin * (1.0 - sigmoid_gate))
        ).astype(jnp.bfloat16)
        up_pre = (hidden_grad * silu_gate).astype(jnp.bfloat16)
        pre[rows, :width] = gate_pre
        pre[rows, width:] = up_pre
        pl.when(g >= 2)(lambda: exchange(g - 2).wait_send())
        for target, at, side in (
            (theirs, group(lax.rem(g, 2)), 1 - core),
            (mine, rows, core),
        ):
            features = pl.ds(pl.multiple_of(side * half, half), half)
            value = dot(gate_pre, gate_w[features], (1, 1)) + dot(up_pre, up_w[features], (1, 1))
            target[at] = value.astype(jnp.bfloat16)
        exchange(g).start()

    def finish(g):
        wait_for(other.at[group(g)], part_recv.at[g])
        rows = group(g)
        mine[rows] = (mine[rows].astype(jnp.float32) + other[rows].astype(jnp.float32)).astype(
            jnp.bfloat16
        )
        for i in range(BLOCKS):
            k = jnp.int32(ORDER[i])
            for later in range(1, GROUPS):
                if later * BLOCKS + i < CHIPS - 1:
                    k = jnp.where(g == later, ORDER[later * BLOCKS + i], k)
            z = lax.rem(me // 16 + 4 - k // 16, 4)
            y = lax.rem(lax.rem(me // 4, 4) + 4 - lax.rem(k // 4, 4), 4)
            x = lax.rem(lax.rem(me, 4) + 4 - lax.rem(k, 4), 4)
            go = remote(
                mine.at[block(g * BLOCKS + i)],
                back.at[block(me)],
                back_send,
                back_recv,
                (z * 16 + y * 4 + x, core),
            )
            if i < BLOCKS - 1:
                go.start()
            else:
                pl.when(g < GROUPS - 1)(go.start)

    def step(i, carry):
        pl.when(i < GROUPS)(lambda: take(i))
        pl.when(i >= 1)(lambda: finish(i - 1))
        pl.when(i < GROUPS)(lambda: compute(i))
        return carry

    lax.fori_loop(0, GROUPS + 1, step, 0)
    back[block(me)] = mine[(CHIPS - 1) * capacity :]

    tile = 128

    def gate_step(i, carry):
        side, at = i // (half // tile), lax.rem(i, half // tile)
        columns = pl.ds(pl.multiple_of(at * tile, tile), tile)
        value = dot(rows_in[side, :, columns], pre[...], (0, 0))
        features = pl.ds(pl.multiple_of(i * tile, tile), tile)
        gate_g[features] = value[:, :width]
        up_g[features] = value[:, width:]
        return carry

    lax.fori_loop(0, D // tile, gate_step, 0)

    def down_step(i, carry):
        side, at = i // 2, lax.rem(i, 2)
        columns = pl.ds(pl.multiple_of(half + at * 512, 512), 512)
        down_g[:, pl.ds(pl.multiple_of(i * 512, 512), 512)] = dot(
            hid[...], rows_in[side, :, columns], (0, 0)
        )
        return carry

    lax.fori_loop(0, 4, down_step, 0)
    sent = (CHIPS - 1) * capacity
    wait_for(back.at[pl.ds(0, sent)], back_recv)
    normed_grad[...] = dot(select[...], back[...], (0, 0))
    wait_for(send.at[pl.ds(0, sent)], send_sem)
    wait_for(mine.at[pl.ds(0, sent)], back_send)
    for g in range(GROUPS):
        passing(g).wait_send()
    for g in range(GROUPS - 2, GROUPS):
        exchange(g).wait_send()


def experts(routes, weights, stream, gain, cot, gate_w, up_w, down_w):
    tokens, half = stream.shape
    slots = 2 * tokens * routes.shape[0]
    width = gate_w.shape[1]
    vmem = pl.BlockSpec(memory_space=pltpu.VMEM)
    hbm = pl.BlockSpec(memory_space=pltpu.HBM)
    f32, bf16 = jnp.float32, jnp.bfloat16
    dma = pltpu.SemaphoreType.DMA
    return pl.pallas_call(
        experts_kernel,
        out_shape=(
            jax.ShapeDtypeStruct((tokens, half), f32),
            jax.ShapeDtypeStruct((tokens, 128), f32),
            jax.ShapeDtypeStruct((D, width), f32),
            jax.ShapeDtypeStruct((D, width), f32),
            jax.ShapeDtypeStruct((width, D), f32),
        ),
        in_specs=[hbm] * 8,
        out_specs=(vmem,) * 5,
        scratch_shapes=[
            pltpu.VMEM(routes.shape, jnp.int32),
            pltpu.VMEM(weights.shape, f32),
            pltpu.VMEM((tokens, half), bf16),
            pltpu.VMEM((1, half), f32),
            pltpu.VMEM((tokens, half), bf16),
            pltpu.VMEM((D, width), bf16),
            pltpu.VMEM((D, width), bf16),
            pltpu.VMEM((width, D), bf16),
            pltpu.VMEM((2, tokens, 128), f32),
            pltpu.VMEM((slots, tokens), bf16),
            pltpu.VMEM((slots, 2 * half), bf16),
            pltpu.VMEM((2, slots, 2 * half), bf16),
            pltpu.VMEM((slots, 2 * width), bf16),
            pltpu.VMEM((slots, width), bf16),
            pltpu.VMEM((2 * slots // GROUPS, half), bf16),
            pltpu.VMEM((slots, half), bf16),
            pltpu.VMEM((slots, half), bf16),
            pltpu.VMEM((slots, half), bf16),
            dma((8,)),
            dma((2,)),
            dma(()),
            dma((GROUPS,)),
            dma((GROUPS,)),
            dma((GROUPS,)),
            dma((GROUPS,)),
            dma((GROUPS,)),
            dma(()),
            dma(()),
        ],
        compiler_params=pltpu.CompilerParams(
            collective_id=0, has_side_effects=True, vmem_limit_bytes=32 << 20
        ),
        name="experts",
    )(
        *(
            pltpu.with_memory_space_constraint(a, pltpu.HBM)
            for a in (routes, weights, stream, gain, cot, gate_w, up_w, down_w)
        )
    )


def tail_kernel(
    normed_grad,
    inverse_in,
    stream,
    gain,
    cot,
    value_in,
    out_gate,
    in_gate,
    taps,
    out_proj,
    stream_grad,
    proj_grad,
    input_grad,
    bgate_grad,
    cgate_grad,
    cross,
    whole,
    rim_in,
    rim_out,
    rim_back,
    conv,
    delta,
    shares,
    got,
    half_sum,
    final,
    cross_sem,
    whole_sem,
    rim_sem,
    back_sem,
    share_send,
    share_recv,
    sum_send,
    sum_recv,
):
    me, core = lax.axis_index("sp"), lax.axis_index("tp")
    partner = (me, 1 - core)
    tokens, half = stream.shape
    barrier = greet_all(me, core)
    stream_float = stream[...].astype(jnp.float32)
    part = jnp.sum(stream_float * gain[...] * normed_grad[...], axis=1, keepdims=True)
    cross[0] = jnp.broadcast_to(part, cross.shape[1:])
    pl.semaphore_wait(barrier, CHIPS)
    swap = remote(cross.at[0], cross.at[1], cross_sem.at[0], cross_sem.at[1], partner)
    swap.start()
    after, ahead = lax.rem(me + 1, CHIPS), lax.rem(me + CHIPS - 1, CHIPS)
    rims = [
        remote(
            ref.at[pl.ds(tokens - 16, 16)],
            rim_in.at[i],
            rim_sem.at[i],
            rim_sem.at[2 + i],
            (after, core),
        )
        for i, ref in enumerate((value_in, in_gate))
    ]
    for rim in rims:
        rim.start()
    swap.wait()
    inverse = inverse_in[:, 0:1]
    total = cross[0, :, 0:1] + cross[1, :, 0:1]
    grad = (
        cot[...].astype(jnp.float32)
        + inverse * gain[...] * normed_grad[...]
        - stream_float * inverse * inverse * inverse * total / D
    ).astype(jnp.bfloat16)
    stream_grad[...] = grad
    whole[core] = grad
    join = remote(
        whole.at[core], whole.at[core], whole_sem.at[0], whole_sem.at[1], partner
    )
    join.start()

    row = lax.broadcasted_iota(jnp.int32, conv.shape, 0)
    gated = in_gate[...].astype(jnp.float32) * value_in[...].astype(jnp.float32)
    for rim in rims:
        rim.wait()
    rim_gated = rim_in[1].astype(jnp.float32) * rim_in[0].astype(jnp.float32)
    rim_gated = jnp.where(me == 0, jnp.zeros_like(rim_gated), rim_gated)
    last, older = rim_gated[15:16], rim_gated[14:15]
    previous = jnp.where(row == 0, last, pltpu.roll(gated, 1, 0))
    before = jnp.where(row == 0, older, jnp.where(row == 1, last, pltpu.roll(gated, 2, 0)))
    conv[...] = taps[0:1] * before + taps[1:2] * previous + taps[2:3] * gated
    mixer_out = (out_gate[...].astype(jnp.float32) * conv[...]).astype(jnp.bfloat16)

    def split(side):
        value = dot(whole[side], mixer_out, (0, 0)).astype(jnp.bfloat16)
        value = value.reshape(2, SIDE, SIDE, 2, 16, value.shape[1])
        for u in range(UNITS):
            r, c = u // 4, u % 4
            shares[u, pl.ds(side * 2, 2)] = value[:, :, :, r, :, c * 128 : (c + 1) * 128]

    split(core)
    wait_for(whole.at[1 - core], whole_sem.at[1])
    split(1 - core)
    here = (me // 16, lax.rem(me // 4, 4), lax.rem(me, 4))

    def at_place(place):
        return (place[0] * 16 + place[1] * 4 + place[2], core)

    def shifted(moves):
        return [lax.rem(h + m, 4) for h, m in zip(here, moves)]

    def plane(u, index):
        first = FIRST[u]
        return shares.at[(u,) + (slice(None),) * first + (index,)]

    for u in UNIT_ORDER:
        for i, step in enumerate((2, 1, 3)):
            place = shifted([step if d == FIRST[u] else 0 for d in range(3)])
            remote(
                plane(u, place[FIRST[u]]),
                got.at[u, i],
                share_send,
                share_recv.at[u],
                at_place(place),
            ).start()
    mixer_grad = dot(whole[0], out_proj[:half]) + dot(whole[1], out_proj[half:])
    delta[...] = mixer_grad * out_gate[...].astype(jnp.float32)
    rim_out[...] = delta[0:8]
    give = remote(rim_out, rim_back, back_sem.at[0], back_sem.at[1], (ahead, core))
    bgate_grad[...] = (mixer_grad * conv[...]).astype(jnp.bfloat16)
    give.start()

    def spread(u):
        rest = [d for d in range(3) if d != FIRST[u]]
        for i, (one, two) in enumerate(PLANE):
            moves = [0, 0, 0]
            moves[rest[0]], moves[rest[1]] = one, two
            place = shifted(moves)
            remote(
                half_sum.at[u, place[rest[0]], place[rest[1]]],
                final.at[u, i],
                sum_send,
                sum_recv.at[u],
                at_place(place),
            ).start()

    earlier = None
    for u in UNIT_ORDER:
        wait_for(got.at[u], share_recv.at[u])
        value = plane(u, here[FIRST[u]])[...].astype(jnp.float32)
        for i in range(SIDE - 1):
            value = value + got[u, i].astype(jnp.float32)
        half_sum[u] = value
        if earlier is not None:
            spread(earlier)
        earlier = u
    spread(earlier)
    give.wait()
    rim_delta = jnp.where(me == CHIPS - 1, jnp.zeros_like(rim_back[...]), rim_back[...])
    nearest, second = rim_delta[0:1], rim_delta[1:2]
    change = delta[...]
    following = jnp.where(row == tokens - 1, nearest, pltpu.roll(change, tokens - 1, 0))
    beyond = jnp.where(
        row == tokens - 2,
        nearest,
        jnp.where(row == tokens - 1, second, pltpu.roll(change, tokens - 2, 0)),
    )
    gated_grad = taps[2:3] * change + taps[1:2] * following + taps[0:1] * beyond
    input_grad[...] = (gated_grad * in_gate[...].astype(jnp.float32)).astype(jnp.bfloat16)
    cgate_grad[...] = (gated_grad * value_in[...].astype(jnp.float32)).astype(jnp.bfloat16)
    for u in UNIT_ORDER:
        rest = [d for d in range(3) if d != FIRST[u]]
        wait_for(final.at[u], sum_recv.at[u])
        total = half_sum[u, here[rest[0]], here[rest[1]]]
        for i in range(len(PLANE)):
            total = total + final[u, i]
        r, c = u // 4, u % 4
        proj_grad[r * 16 : (r + 1) * 16, c * 128 : (c + 1) * 128] = total
    wait_for(got, share_send)
    wait_for(final, sum_send)
    wait_for(whole.at[core], whole_sem.at[0])


def tail(normed_grad, inverse, stream, gain, cot, value_in, out_gate, in_gate, taps, out_proj):
    tokens, half = stream.shape
    width = value_in.shape[1]
    height = D // CHIPS
    vmem = pl.BlockSpec(memory_space=pltpu.VMEM)
    f32, bf16 = jnp.float32, jnp.bfloat16
    dma = pltpu.SemaphoreType.DMA
    return pl.pallas_call(
        tail_kernel,
        out_shape=(
            jax.ShapeDtypeStruct((tokens, half), bf16),
            jax.ShapeDtypeStruct((height, width), f32),
            jax.ShapeDtypeStruct((tokens, width), bf16),
            jax.ShapeDtypeStruct((tokens, width), bf16),
            jax.ShapeDtypeStruct((tokens, width), bf16),
        ),
        in_specs=[vmem] * 10,
        out_specs=(vmem,) * 5,
        scratch_shapes=[
            pltpu.VMEM((2, tokens, 128), f32),
            pltpu.VMEM((2, tokens, half), bf16),
            pltpu.VMEM((2, 16, width), bf16),
            pltpu.VMEM((8, width), f32),
            pltpu.VMEM((8, width), f32),
            pltpu.VMEM((tokens, width), f32),
            pltpu.VMEM((tokens, width), f32),
            pltpu.VMEM((UNITS, SIDE, SIDE, SIDE, 16, 128), bf16),
            pltpu.VMEM((UNITS, SIDE - 1, SIDE, SIDE, 16, 128), bf16),
            pltpu.VMEM((UNITS, SIDE, SIDE, 16, 128), f32),
            pltpu.VMEM((UNITS, len(PLANE), 16, 128), f32),
            dma((2,)),
            dma((2,)),
            dma((4,)),
            dma((2,)),
            dma(()),
            dma((UNITS,)),
            dma(()),
            dma((UNITS,)),
        ],
        compiler_params=pltpu.CompilerParams(
            collective_id=1, has_side_effects=True, vmem_limit_bytes=12 << 20
        ),
        name="tail",
    )(normed_grad, inverse, stream, gain, cot, value_in, out_gate, in_gate, taps, out_proj)


def store_kernel(*refs):
    count = len(refs) // 2
    sem = refs[-1]
    copies = [
        pltpu.make_async_copy(refs[i], refs[count + i], sem.at[i]) for i in range(count)
    ]
    for copy in copies:
        copy.start()
    for copy in copies:
        copy.wait()


def store(*arrays):
    return pl.pallas_call(
        store_kernel,
        out_shape=tuple(jax.ShapeDtypeStruct(a.shape, a.dtype) for a in arrays),
        in_specs=[pl.BlockSpec(memory_space=pltpu.VMEM)] * len(arrays),
        out_specs=(pl.BlockSpec(memory_space=pltpu.HBM),) * len(arrays),
        scratch_shapes=[pltpu.SemaphoreType.DMA((len(arrays),))],
        compiler_params=pltpu.CompilerParams(vmem_limit_bytes=1 << 20),
        name="store",
    )(*arrays)


def local(
    stream,
    norm_gain,
    cotangent,
    route_weights,
    routes,
    conv_input,
    conv_bgate,
    conv_cgate,
    conv_taps,
    out_proj,
    gate_weight,
    up_weight,
    down_weight,
):
    gain = norm_gain[None, :]
    normed_grad, inverse, gate_g, up_g, down_g = experts(
        routes.T,
        route_weights.T,
        stream,
        gain,
        cotangent,
        gate_weight[0],
        up_weight[0],
        down_weight[0],
    )
    stream_grad, proj_grad, input_grad, bgate_grad, cgate_grad = tail(
        normed_grad,
        inverse,
        stream,
        gain,
        cotangent,
        conv_input,
        conv_bgate,
        conv_cgate,
        conv_taps,
        out_proj,
    )
    outs = store(
        stream_grad, proj_grad, input_grad, bgate_grad, cgate_grad, gate_g, up_g, down_g
    )
    return (*outs[:5], *(out[None] for out in outs[5:]))


def solution(mesh):
    return jax.shard_map(
        local,
        mesh=mesh,
        in_specs=(
            P("sp", "tp"),
            P("tp"),
            P("sp", "tp"),
            P("sp", None),
            P("sp", None),
            P("sp", "tp"),
            P("sp", "tp"),
            P("sp", "tp"),
            P(None, "tp"),
            P(None, "tp"),
            P("sp", None, "tp"),
            P("sp", None, "tp"),
            P("sp", "tp", None),
        ),
        out_specs=(
            P("sp", "tp"),
            P("sp", "tp"),
            P("sp", "tp"),
            P("sp", "tp"),
            P("sp", "tp"),
            P("sp", None, "tp"),
            P("sp", None, "tp"),
            P("sp", "tp", None),
        ),
        check_vma=False,
    )
```
